256 devices in a mesh: kv: 32 (over z, x), tp: 8 (over y, core).
Axes of the slice: x: 4, y: 4, z: 8, core: 2. Of those that a mesh axis runs over, the one named last changes fastest.
Arguments:
- tokens: bfloat16 [4096, 2048], P('kv', 'tp'), may hold values from -6 to 6
- states: float32 [4096, 16, 64, 64], P('kv', 'tp'), may hold values from -6 to 6
- mix_gain: bfloat16 [2048], replicated, may hold values from 0.099609375 to 1.8984375
- w_query: bfloat16 [2048, 1024], P(None, 'tp'), may hold values from -0.125 to 0.125
- w_key: bfloat16 [2048, 1024], P(None, 'tp'), may hold values from -0.125 to 0.125
- w_value: bfloat16 [2048, 1024], P(None, 'tp'), may hold values from -0.125 to 0.125
- w_gate: bfloat16 [2048, 1024], P(None, 'tp'), may hold values from -0.125 to 0.125
- head_gain: bfloat16 [1024], P('tp'), may hold values from 0.099609375 to 1.8984375
- w_output: bfloat16 [1024, 2048], P('tp'), may hold values from -0.1875 to 0.1875
- channel_gain: bfloat16 [2048], replicated, may hold values from 0.099609375 to 1.8984375
- w_up: bfloat16 [2048, 8192], P(None, 'kv'), may hold values from -0.125 to 0.125
- w_down: bfloat16 [8192, 2048], P('kv'), may hold values from -0.0625 to 0.0625
Outputs:
- layer_out: bfloat16 [4096, 2048], P('kv', 'tp')
- new_states: float32 [4096, 16, 64, 64], P('kv', 'tp')
The draws below stay inside these ranges and needn't reach their ends.
All inputs are finite; a program needn't handle non-finite values.
Results may differ from the reference program's by a relative error of at most 0.019.
Values may be sent and summed in bfloat16 or wider, within the bound.
A program may use at most 64 MiB of HBM per device.

```python
import jax
import jax.numpy as jnp
from jax import lax

D = 2048
HEADS = 16
HEAD = 64
FF = 8192
POS = 16384
BATCH = 4096
N_TP = 8


def draw_tokens(key, part):
    first_key = jax.random.fold_in(jax.random.fold_in(key, 11), 0)
    column = jnp.arange(D, dtype=jnp.float32) / D
    profile = 0.5 * jnp.exp(jnp.log(3.0) * column)
    drawn = jax.random.normal(first_key, (BATCH, D), jnp.float32) * profile
    return jnp.clip(drawn, -6.0, 6.0).astype(jnp.bfloat16)


def shard_levels(rng, extent, shards, smallest, high):
    gain = 1.0
    for dim, parts in shards:
        steps = jax.random.uniform(jax.random.fold_in(jax.random.fold_in(rng, 6), dim), (parts,), jnp.float32, smallest / len(shards), high / len(shards))
        gain = gain * jnp.repeat(jnp.exp(steps), extent[dim] // parts).reshape((-1,) + (1,) * (len(extent) - 1 - dim))
    return gain


def scatter_about(rng, extent, scale, bound, shards=(), kind=jnp.bfloat16):
    array = jax.random.normal(rng, extent, jnp.float32) * scale
    if len(shards) > 0:
        array = shard_levels(rng, extent, shards, -0.22, 0.18) * array
    return jnp.clip(array, min=-bound, max=bound).astype(kind)


def setup_inputs(seed: int = 0) -> dict:
    arg_keys = jax.random.split(jax.random.key(seed), 13)
    return {
        "tokens": draw_tokens(jax.random.fold_in(arg_keys[12], 71), 0),
        "states": scatter_about(arg_keys[1], (BATCH, HEADS, HEAD, HEAD), 1.0, 6.0, ((0, 32), (1, 8)), jnp.float32),
        "mix_gain": jnp.clip(1.0 + 0.18 * jax.random.normal(arg_keys[2], (D,), jnp.float32), 0.099609375, 1.8984375).astype(jnp.bfloat16),
        "w_query": scatter_about(arg_keys[3], (D, HEADS * HEAD), D ** -0.5, 0.125, ((1, 8),)),
        "w_key": scatter_about(arg_keys[4], (D, HEADS * HEAD), D ** -0.5, 0.125, ((1, 8),)),
        "w_value": scatter_about(arg_keys[5], (D, HEADS * HEAD), D ** -0.5, 0.125, ((1, 8),)),
        "w_gate": scatter_about(arg_keys[6], (D, HEADS * HEAD), D ** -0.5, 0.125, ((1, 8),)),
        "head_gain": jnp.clip(1.0 + 0.18 * jax.random.normal(arg_keys[7], (HEADS * HEAD,), jnp.float32), 0.099609375, 1.8984375).astype(jnp.bfloat16),
        "w_output": scatter_about(arg_keys[8], (HEADS * HEAD, D), (HEADS * HEAD) ** -0.5, 0.1875, ((0, 8),)),
        "channel_gain": jnp.clip(1.0 + 0.18 * jax.random.normal(arg_keys[9], (D,), jnp.float32), 0.099609375, 1.8984375).astype(jnp.bfloat16),
        "w_up": scatter_about(arg_keys[10], (D, FF), D ** -0.5, 0.125, ((1, 32),)),
        "w_down": scatter_about(arg_keys[11], (FF, D), FF ** -0.5, 0.0625, ((0, 32),)),
    }


EPSILON = 1e-06
ROTARY_BASE = 10000.0

def rotate(vectors):
    half_size = vectors.shape[-1] // 2
    frequency = ROTARY_BASE ** (-jnp.arange(half_size, dtype=jnp.float32) / half_size)
    angles = POS * frequency
    cosine = jnp.cos(angles)
    sines = jnp.sin(angles)
    first_half = vectors[..., :half_size]
    second = vectors[..., half_size:]
    return jnp.concatenate([first_half * cosine - second * sines, first_half * sines + second * cosine], axis=-1)

def retain(normed, states, w_query, w_key, w_value, w_gate, head_gain, head_ids):
    row_count = states.shape[0]
    head_count = states.shape[1]
    head_size = states.shape[2]

    def project(weight):
        return jnp.dot(normed, weight, preferred_element_type=jnp.float32).reshape(row_count, head_count, head_size)
    queries = rotate(project(w_query)) * head_size ** (-0.5)
    keys_now = rotate(project(w_key))
    values = project(w_value)
    gating = jnp.dot(normed, w_gate, preferred_element_type=jnp.float32)
    decays = 1.0 - jnp.exp2(-1.0 - 11.0 * head_ids / (HEADS - 1))
    new_states = decays[None, :, None, None] * states + keys_now[:, :, :, None] * values[:, :, None, :]
    output = jnp.einsum('bhk,bhkv->bhv', queries, new_states, precision=lax.Precision.HIGHEST)
    center = output - lax.optimization_barrier(jnp.mean(output, axis=-1, keepdims=True))
    spread = lax.optimization_barrier(jnp.mean(center * center, axis=-1, keepdims=True))
    scaled = center * lax.rsqrt(spread + EPSILON) * head_gain.astype(jnp.float32).reshape(head_count, head_size)
    gated_out = (scaled.reshape(row_count, head_count * head_size) * jax.nn.silu(gating)).astype(jnp.bfloat16)
    return (gated_out, new_states)

def reference(tokens, states, mix_gain, w_query, w_key, w_value, w_gate, head_gain, w_output, channel_gain, w_up, w_down):
    widened = tokens.astype(jnp.float32)
    inverse_rms = lax.rsqrt(lax.optimization_barrier(jnp.mean(widened * widened, axis=1, keepdims=True)) + EPSILON)
    normed = (widened * inverse_rms * mix_gain.astype(jnp.float32)).astype(jnp.bfloat16)
    head_ids = jnp.arange(HEADS).astype(jnp.float32)
    gated_out, new_states = retain(normed, states, w_query, w_key, w_value, w_gate, head_gain, head_ids)
    blocks = gated_out.astype(jnp.float32).reshape(BATCH, N_TP, -1)
    weights = w_output.astype(jnp.float32).reshape(N_TP, -1, D)
    partials = jnp.einsum('btc,tcd->btd', blocks, weights)
    rounded = lax.optimization_barrier(partials.astype(jnp.bfloat16))
    attended = lax.optimization_barrier(jnp.sum(rounded.astype(jnp.float32), axis=1))
    middle = (widened + attended).astype(jnp.bfloat16)
    mid_wide = middle.astype(jnp.float32)
    second_rms = lax.rsqrt(lax.optimization_barrier(jnp.mean(mid_wide * mid_wide, axis=1, keepdims=True)) + EPSILON)
    scaled = (mid_wide * channel_gain.astype(jnp.float32)).astype(jnp.bfloat16)
    hidden = jnp.dot(scaled, w_up, preferred_element_type=jnp.float32) * second_rms
    activated = jnp.square(jax.nn.relu(hidden)).astype(jnp.bfloat16)
    down_sum = jnp.dot(activated, w_down, preferred_element_type=jnp.float32)
    layer_out = (mid_wide + down_sum).astype(jnp.bfloat16)
    return (layer_out, new_states)
```

```python
import functools

import jax
import jax.numpy as jnp
from jax import lax
from jax.experimental import pallas as pl
from jax.experimental.pallas import tpu as pltpu
from jax.sharding import Mesh
from jax.sharding import PartitionSpec as P

HEADS = 16
POS = 16384
KV = ("z", "x")
TP = ("y", "c")

EPSILON = 1e-06
ROTARY_BASE = 10000.0

D = 2048
W1 = 768
SIZES = {"z": 8, "x": 4, "y": 4, "c": 2}
F32 = jnp.float32
BF16 = jnp.bfloat16


def slot(offset):
    return 2 * abs(offset) - (1 if offset > 0 else 0)


def last(n):
    return n - 1


class Copies:
    def __init__(self, send_sem, recv_sem):
        self.send_sem, self.recv_sem, self.made = send_sem, recv_sem, []

    def make(self, src, dst, axis, step):
        n = SIZES[axis]
        index = len(self.made)
        copy = pltpu.make_async_remote_copy(
            src_ref=src,
            dst_ref=dst,
            send_sem=self.send_sem.at[index],
            recv_sem=self.recv_sem.at[index],
            device_id={axis: lax.rem(lax.axis_index(axis) + (step + n), n)},
            device_id_type=pl.DeviceIdType.MESH,
        )
        self.made.append(copy)
        return copy

    def send(self, *args):
        copy = self.make(*args)
        copy.start()
        return copy

    def finish(self):
        for copy in self.made:
            copy.wait_send()


def greet(peers):
    barrier = pltpu.get_barrier_semaphore()
    for peer in peers:
        pl.semaphore_signal(barrier, inc=1, device_id=peer, device_id_type=pl.DeviceIdType.MESH)
    return barrier


def neighbour(axis, step):
    n = SIZES[axis]
    return {axis: lax.rem(lax.axis_index(axis) + (step + n), n)}


def half(start, stop, step):
    middle = (start + stop) // 2
    return slice(start, middle) if step > 0 else slice(middle, stop)


def gather_kernel(tok_ref, out_ref, send_sem, recv_sem):
    y, c = lax.axis_index("y"), lax.axis_index("c")
    barrier = greet([neighbour("y", 1), neighbour("y", -1), neighbour("c", 1)])
    out_ref[2 * y + c] = tok_ref[...]
    pl.semaphore_wait(barrier, 3)
    copies = Copies(send_sem, recv_sem)
    rows = tok_ref.shape[0]

    def block(step):
        return 2 * lax.rem(y + (step + 4), 4) + c

    near = {}
    for step in (1, -1):
        near[step] = copies.send(tok_ref, out_ref.at[2 * y + c], "y", step)
    across = [copies.send(tok_ref, out_ref.at[2 * y + c], "c", 1)]
    far = {}
    for step in (1, -1):
        near[step].wait_recv()
        mine = block(-step)
        part = half(0, rows, step)
        far[step] = copies.send(out_ref.at[mine, part], out_ref.at[mine, part], "y", step)
        across.append(copies.send(out_ref.at[mine], out_ref.at[mine], "c", 1))
    for step in (1, -1):
        far[step].wait_recv()
        mine = block(2)
        part = half(0, rows, step)
        across.append(copies.send(out_ref.at[mine, part], out_ref.at[mine, part], "c", 1))
    for copy in across:
        copy.wait_recv()
    copies.finish()


def gather_tokens(tokens):
    rows, width = tokens.shape
    return pl.pallas_call(
        gather_kernel,
        out_shape=jax.ShapeDtypeStruct((8, rows, width), tokens.dtype),
        in_specs=[pl.BlockSpec(memory_space=pltpu.VMEM)],
        out_specs=pl.BlockSpec(memory_space=pltpu.VMEM),
        scratch_shapes=[pltpu.SemaphoreType.DMA((16,)), pltpu.SemaphoreType.DMA((16,))],
        compiler_params=pltpu.CompilerParams(
            collective_id=0, has_side_effects=True, vmem_limit_bytes=4 * 2**20
        ),
        name="gather_tokens",
    )(tokens)


def mixer_kernel(
    part_ref,
    own_ref,
    gain_ref,
    up_hbm,
    down_hbm,
    out_ref,
    up_ref,
    down_ref,
    xs,
    ps,
    pair_in,
    y_sum,
    y_far_in,
    y_near_in,
    mid,
    fin,
    z1_in,
    x1_far_in,
    x1_near_in,
    x2_far_in,
    x2_near_in,
    z2_in,
    load_sem,
    send_sem,
    recv_sem,
):
    y, c = lax.axis_index("y"), lax.axis_index("c")
    tp = 2 * y + c
    peers = [{"y": lax.rem(y + dy, 4), "c": lax.rem(c + dc, 2)} for dy in range(4) for dc in range(2) if dy or dc]
    ring = [neighbour(axis, step) for axis in ("z", "x") for step in (1, -1)]
    barrier = greet(peers + ring)
    load_up = pltpu.make_async_copy(up_hbm, up_ref, load_sem.at[0])
    load_down = pltpu.make_async_copy(down_hbm, down_ref, load_sem.at[1])
    load_up.start()
    load_down.start()
    pl.semaphore_wait(barrier, len(peers) + len(ring))

    copies = Copies(send_sem, recv_sem)
    send = copies.send
    both = (1, -1)

    def rows_for(offset, core):
        return 2 * lax.rem(y + (offset + 4), 4) + core

    offsets = {3: 2, 1: 1, 2: -1, 0: 0}
    across = {}
    for s in (3, 1, 2, 0):
        across[s] = send(part_ref.at[rows_for(offsets[s], 1 - c)], pair_in.at[s], "c", 1)

    def pair_sum(s):
        across[s].wait_recv()
        return part_ref[rows_for(offsets[s], c)].astype(F32) + pair_in[s].astype(F32)

    y_sum[3] = pair_sum(3).astype(BF16)
    far = {}
    for step in both:
        cols = half(0, D, step)
        far[step] = send(y_sum.at[3, :, cols], y_far_in.at[slot(step)], "y", step)
    near = {}
    for step in both:
        s = slot(step)
        cols = half(0, D, step)
        total = pair_sum(s)
        y_sum[s] = total.astype(BF16)
        far[step].wait_recv()
        y_sum[s, :, cols] = (total[:, cols] + y_far_in[s].astype(F32)).astype(BF16)
        near[step] = send(y_sum.at[s], y_near_in.at[s - 1], "y", step)
    attended = pair_sum(0)
    for step in both:
        near[step].wait_recv()
        attended = attended + y_near_in[slot(step) - 1].astype(F32)
    middle = (own_ref[...].astype(F32) + attended).astype(BF16)
    xs[0, 0] = middle
    mid[...] = middle

    c1, c2 = (0, W1), (W1, D)
    full1, full2 = slice(*c1), slice(*c2)
    batches = {"A": slice(0, 1), "B": slice(1, 3), "C": slice(3, 4)}

    def z_hop1(name, step, hop):
        r = batches[name]
        cols = full1 if hop < 4 else half(*c1, step)
        return send(
            xs.at[slot(-step * (hop - 1)), r, :, cols],
            xs.at[slot(-step * hop) if hop < 4 else 7, r, :, cols],
            "z",
            step,
        )

    def z_hop2(step, hop):
        cols = full2 if hop < 4 else half(*c2, step)
        return send(
            xs.at[slot(-step * (hop - 1)), 0, :, cols],
            xs.at[slot(-step * hop) if hop < 4 else 7, 0, :, cols],
            "z",
            step,
        )

    def z_slots(k):
        return slice(0, 1) if k == 0 else slice(7, 8) if k == 4 else slice(2 * k - 1, 2 * k + 1)

    def x_near2(k, step):
        r = z_slots(k)
        return send(xs.at[r, 0, :, full2], xs.at[r, slot(-step), :, full2], "x", step)

    def x_far2(k, step):
        r, cols = z_slots(k), half(*c2, step)
        return send(xs.at[r, slot(-step), :, cols], xs.at[r, 3, :, cols], "x", step)

    x_near1 = {s: send(xs.at[0, 0, :, full1], xs.at[0, slot(-s), :, full1], "x", s) for s in both}
    z2 = {(s, 1): z_hop2(s, 1) for s in both}
    x2n = {(0, s): x_near2(0, s) for s in both}
    z1 = {("A", s, 1): z_hop1("A", s, 1) for s in both}
    x2f = {}

    load_up.wait()
    load_down.wait()

    def mix(k):
        r = z_slots(k)
        n = (r.stop - r.start) * 64
        rows = xs[r].reshape(n, D).astype(F32)
        second_rms = lax.rsqrt(jnp.mean(rows * rows, axis=1, keepdims=True) + EPSILON)
        scaled = (rows * gain_ref[...].astype(F32)).astype(BF16)
        hidden = jnp.dot(scaled, up_ref[...], preferred_element_type=F32) * second_rms
        activated = jnp.square(jnp.maximum(hidden, 0.0)).astype(BF16)
        result = jnp.dot(activated, down_ref[...], preferred_element_type=F32).astype(BF16)
        ps[r] = result.reshape(r.stop - r.start, 4, 16, D)

    x_far1 = {}
    for s in both:
        x_near1[s].wait_recv()
        cols = half(*c1, s)
        x_far1[s] = send(xs.at[0, slot(-s), :, cols], xs.at[0, 3, :, cols], "x", s)
    for s in both:
        z1["B", s, 1] = z_hop1("B", s, 1)

    for level in range(1, 7):
        if level <= 4:
            for s in both:
                z2[s, level].wait_recv()
                if level < 4:
                    z2[s, level + 1] = z_hop2(s, level + 1)
            for s in both:
                x2n[level, s] = x_near2(level, s)
        if level == 2:
            for s in both:
                x_far1[s].wait_recv()
            for s in both:
                z1["C", s, 1] = z_hop1("C", s, 1)
        for name, behind in (("A", 0), ("B", 1), ("C", 2)):
            hop = level - behind
            if 1 <= hop <= 4:
                for s in both:
                    z1[name, s, hop].wait_recv()
                    if hop < 4:
                        z1[name, s, hop + 1] = z_hop1(name, s, hop + 1)
        if level <= 5:
            for s in both:
                x2n[level - 1, s].wait_recv()
                x2f[level - 1, s] = x_far2(level - 1, s)
        if level >= 2:
            for s in both:
                x2f[level - 2, s].wait_recv()
            mix(level - 2)

    def add(index, arrived):
        ps[index] = (ps[index].astype(F32) + arrived.astype(F32)).astype(BF16)

    def x_out_far2(k, s):
        r, cols = z_slots(k), half(*c2, s)
        return send(ps.at[r, 3, :, cols], x2_far_in.at[r, slot(s) - 1], "x", s)

    def x_out_near2(k, s):
        r = z_slots(k)
        return send(ps.at[r, slot(s), :, full2], x2_near_in.at[r, slot(s) - 1], "x", s)

    def z_out1(name, s, hop):
        r = batches[name]
        if hop == 4:
            cols = half(*c1, s)
            return send(ps.at[7, r, :, cols], z1_in.at[slot(s) - 1, 3, r, :, cols], "z", s)
        return send(ps.at[slot(s * hop), r, :, full1], z1_in.at[slot(s) - 1, hop - 1, r, :, full1], "z", s)

    def z_out2(s, hop):
        if hop == 4:
            cols = half(0, D - W1, s)
            return send(ps.at[7, 0, :, half(*c2, s)], z2_in.at[slot(s) - 1, 3, :, cols], "z", s)
        return send(ps.at[slot(s * hop), 0, :, full2], z2_in.at[slot(s) - 1, hop - 1], "z", s)

    def take_far2(k):
        r = z_slots(k)
        for s in both:
            of[k, s].wait_recv()
            add((r, slot(s), slice(None), half(*c2, s)), x2_far_in[r, slot(s) - 1])
            on[k, s] = x_out_near2(k, s)

    def take_near2(k):
        r = z_slots(k)
        for s in both:
            on[k, s].wait_recv()
        arrived = x2_near_in[r, 0].astype(F32) + x2_near_in[r, 1].astype(F32)
        add((r, 0, slice(None), full2), arrived)

    of, on, oz1, oz2 = {}, {}, {}, {}
    for name in ("C", "B", "A"):
        for s in both:
            oz1[name, s, 4] = z_out1(name, s, 4)
    for k in (4, 3, 2):
        for s in both:
            of[k, s] = x_out_far2(k, s)

    def pass_on1(hop):
        for name in ("C", "B", "A"):
            r = batches[name]
            for s in both:
                oz1[name, s, hop + 1].wait_recv()
                cols = half(*c1, s) if hop == 3 else full1
                add((slot(s * hop), r, slice(None), cols), z1_in[slot(s) - 1, hop, r, :, cols])
                oz1[name, s, hop] = z_out1(name, s, hop)

    def pass_on2(hop):
        for s in both:
            oz2[s, hop + 1].wait_recv()
            if hop == 3:
                arrived = z2_in[slot(s) - 1, 3, :, half(0, D - W1, s)]
                add((slot(s * 3), 0, slice(None), half(*c2, s)), arrived)
            else:
                add((slot(s * hop), 0, slice(None), full2), z2_in[slot(s) - 1, hop])
            oz2[s, hop] = z_out2(s, hop)

    take_far2(4)
    pass_on1(3)
    take_far2(3)
    for k in (1, 0):
        for s in both:
            of[k, s] = x_out_far2(k, s)
    take_near2(4)
    for s in both:
        oz2[s, 4] = z_out2(s, 4)
    pass_on1(2)
    take_near2(3)
    take_far2(2)
    pass_on2(3)
    pass_on1(1)
    take_near2(2)
    take_far2(1)
    pass_on2(2)
    for name in ("C", "B", "A"):
        r = batches[name]
        for s in both:
            oz1[name, s, 1].wait_recv()
        arrived = z1_in[0, 0, r, :, full1].astype(F32) + z1_in[1, 0, r, :, full1].astype(F32)
        add((0, r, slice(None), full1), arrived)
        if name == "C":
            far1 = {}
            for s in both:
                far1[s] = send(ps.at[0, 3, :, half(*c1, s)], x1_far_in.at[slot(s) - 1], "x", s)
    take_near2(1)
    take_far2(0)
    pass_on2(1)
    near1 = {}
    for s in both:
        far1[s].wait_recv()
        add((0, slot(s), slice(None), half(*c1, s)), x1_far_in[slot(s) - 1])
        near1[s] = send(ps.at[0, slot(s), :, full1], x1_near_in.at[slot(s) - 1], "x", s)
    take_near2(0)
    down2 = ps[0, 0, :, full2].astype(F32)
    for s in both:
        oz2[s, 1].wait_recv()
        down2 = down2 + z2_in[slot(s) - 1, 0].astype(F32)
    down1 = ps[0, 0, :, full1].astype(F32)
    for s in both:
        near1[s].wait_recv()
        down1 = down1 + x1_near_in[slot(s) - 1].astype(F32)
    fin[:, full2] = (mid[:, full2].astype(F32) + down2).astype(BF16)
    fin[:, full1] = (mid[:, full1].astype(F32) + down1).astype(BF16)

    width = out_ref.shape[2]

    def features(index):
        return pl.ds(pl.multiple_of(index * width, width), width)

    back = []
    index = len(copies.made)
    for peer in peers:
        other = 2 * peer["y"] + peer["c"]
        copy = pltpu.make_async_remote_copy(
            src_ref=fin.at[:, features(other)],
            dst_ref=out_ref.at[tp],
            send_sem=send_sem.at[index],
            recv_sem=recv_sem.at[index],
            device_id=peer,
            device_id_type=pl.DeviceIdType.MESH,
        )
        copy.start()
        back.append(copy)
        index += 1
    out_ref[tp] = fin[:, features(tp)]
    for copy in back:
        copy.wait_recv()
    for copy in back:
        copy.wait_send()
    copies.finish()


def mix_channels(partial, own_rows, channel_gain, w_up, w_down):
    vmem = pl.BlockSpec(memory_space=pltpu.VMEM)
    anywhere = pl.BlockSpec(memory_space=pl.ANY)
    hidden = w_up.shape[1]
    w2 = D - W1
    copies = 160
    return pl.pallas_call(
        mixer_kernel,
        out_shape=jax.ShapeDtypeStruct((8, 16, 256), BF16),
        in_specs=[vmem, vmem, vmem, anywhere, anywhere],
        out_specs=vmem,
        scratch_shapes=[
            pltpu.VMEM((D, hidden), BF16),
            pltpu.VMEM((hidden, D), BF16),
            pltpu.VMEM((8, 4, 16, D), BF16),
            pltpu.VMEM((8, 4, 16, D), BF16),
            pltpu.VMEM((4, 16, D), BF16),
            pltpu.VMEM((4, 16, D), BF16),
            pltpu.VMEM((3, 16, D // 2), BF16),
            pltpu.VMEM((2, 16, D), BF16),
            pltpu.VMEM((16, D), BF16),
            pltpu.VMEM((16, D), BF16),
            pltpu.VMEM((2, 4, 4, 16, W1), BF16),
            pltpu.VMEM((2, 16, W1 // 2), BF16),
            pltpu.VMEM((2, 16, W1), BF16),
            pltpu.VMEM((8, 2, 16, w2 // 2), BF16),
            pltpu.VMEM((8, 2, 16, w2), BF16),
            pltpu.VMEM((2, 4, 16, w2), BF16),
            pltpu.SemaphoreType.DMA((2,)),
            pltpu.SemaphoreType.DMA((copies,)),
            pltpu.SemaphoreType.DMA((copies,)),
        ],
        compiler_params=pltpu.CompilerParams(
            collective_id=1, has_side_effects=True, vmem_limit_bytes=40 * 2**20
        ),
        name="mix_channels",
    )(partial.reshape(8, 16, D), own_rows, channel_gain.reshape(1, D), w_up, w_down)


def rotate(vectors):
    half_size = vectors.shape[-1] // 2
    frequency = ROTARY_BASE ** (-jnp.arange(half_size, dtype=F32) / half_size)
    angles = POS * frequency
    cosine = jnp.cos(angles)
    sines = jnp.sin(angles)
    first_half = vectors[..., :half_size]
    second = vectors[..., half_size:]
    return jnp.concatenate(
        [first_half * cosine - second * sines, first_half * sines + second * cosine], axis=-1
    )


def retain(normed, states, w_query, w_key, w_value, w_gate, head_gain, head_ids):
    row_count = states.shape[0]
    head_count = states.shape[1]
    head_size = states.shape[2]

    def project(weight):
        return jnp.dot(normed, weight, preferred_element_type=F32).reshape(
            row_count, head_count, head_size
        )

    queries = rotate(project(w_query)) * head_size ** (-0.5)
    keys_now = rotate(project(w_key))
    values = project(w_value)
    gating = jnp.dot(normed, w_gate, preferred_element_type=F32)
    decays = 1.0 - jnp.exp2(-1.0 - 11.0 * head_ids / (HEADS - 1))
    new_states = (
        decays[None, :, None, None] * states + keys_now[:, :, :, None] * values[:, :, None, :]
    )
    output = jnp.einsum("bhk,bhkv->bhv", queries, new_states, precision=lax.Precision.HIGHEST)
    center = output - jnp.mean(output, axis=-1, keepdims=True)
    spread = jnp.mean(center * center, axis=-1, keepdims=True)
    scaled = (
        center
        * lax.rsqrt(spread + EPSILON)
        * head_gain.astype(F32).reshape(head_count, head_size)
    )
    gated_out = (scaled.reshape(row_count, head_count * head_size) * jax.nn.silu(gating)).astype(
        BF16
    )
    return (gated_out, new_states)


def local(
    tokens,
    states,
    mix_gain,
    w_query,
    w_key,
    w_value,
    w_gate,
    head_gain,
    w_output,
    channel_gain,
    w_up,
    w_down,
):
    blocks = gather_tokens(tokens)
    full_rows = jnp.moveaxis(blocks, 0, 1).reshape(tokens.shape[0], D)
    widened = full_rows.astype(F32)
    inverse_rms = lax.rsqrt(jnp.mean(widened * widened, axis=1, keepdims=True) + EPSILON)
    normed = (widened * inverse_rms * mix_gain.astype(F32)).astype(BF16)
    local_heads = states.shape[1]
    tp_index = lax.axis_index(TP)
    head_ids = (tp_index * local_heads + jnp.arange(local_heads)).astype(F32)
    gated_out, new_states = retain(
        normed, states, w_query, w_key, w_value, w_gate, head_gain, head_ids
    )
    partial_value = jnp.dot(gated_out, w_output, preferred_element_type=F32).astype(BF16)
    own_rows = lax.dynamic_slice_in_dim(full_rows, tp_index * 16, 16, 0)
    out = mix_channels(partial_value, own_rows, channel_gain, w_up, w_down)
    return (out.reshape(128, 256), new_states)


def solution(mesh):
    torus = Mesh(mesh.devices.reshape(8, 4, 4, 2), ("z", "x", "y", "c"))
    in_specs = (
        P(KV, TP),
        P(KV, TP, None, None),
        P(),
        P(None, TP),
        P(None, TP),
        P(None, TP),
        P(None, TP),
        P(TP),
        P(TP, None),
        P(),
        P(None, KV),
        P(KV, None),
    )
    out_specs = (P(KV, TP), P(KV, TP, None, None))
    return jax.shard_map(local, mesh=torus, in_specs=in_specs, out_specs=out_specs, check_vma=False)
```

```python
import jax
import jax.numpy as jnp
import numpy as np
from jax import lax
from jax.experimental import pallas as pl
from jax.experimental.pallas import tpu as pltpu
from jax.sharding import Mesh
from jax.sharding import PartitionSpec as P

HEADS = 16
POS = 16384
KV = ("z", "x")
TP = ("y", "c")

EPSILON = 1e-06
ROTARY_BASE = 10000.0

D = 2048
SIZES = {"z": 8, "x": 4, "y": 4, "c": 2}
F32 = jnp.float32
BF16 = jnp.bfloat16


def slot(offset):
    return 2 * abs(offset) - (1 if offset > 0 else 0)


class Copies:
    def __init__(self, send_sem, recv_sem):
        self.send_sem, self.recv_sem, self.made = send_sem, recv_sem, []

    def send_to(self, src, dst, device):
        index = len(self.made)
        copy = pltpu.make_async_remote_copy(
            src_ref=src,
            dst_ref=dst,
            send_sem=self.send_sem.at[index],
            recv_sem=self.recv_sem.at[index],
            device_id=device,
            device_id_type=pl.DeviceIdType.MESH,
        )
        copy.start()
        self.made.append(copy)
        return copy

    def send(self, src, dst, axis, step):
        return self.send_to(src, dst, neighbour(axis, step))

    def finish(self):
        for copy in self.made:
            copy.wait_send()


def greet(peers):
    barrier = pltpu.get_barrier_semaphore()
    for peer in peers:
        pl.semaphore_signal(barrier, inc=1, device_id=peer, device_id_type=pl.DeviceIdType.MESH)
    return barrier


def neighbour(axis, step):
    n = SIZES[axis]
    return {axis: lax.rem(lax.axis_index(axis) + (step + n), n)}


def half(start, stop, step):
    middle = (start + stop) // 2
    return slice(start, middle) if step > 0 else slice(middle, stop)


def layer_kernel(
    tok_hbm,
    states_hbm,
    mix_gain_hbm,
    wq_hbm,
    wk_hbm,
    wv_hbm,
    wg_hbm,
    head_gain_hbm,
    wo_hbm,
    channel_gain_hbm,
    up_hbm,
    down_hbm,
    turn_hbm,
    out_ref,
    new_ref,
    mix_gain_ref,
    head_gain_ref,
    channel_gain_ref,
    turn_ref,
    blocks,
    w_ref,
    wo_ref,
    states,
    normed,
    q_t,
    k_t,
    gated_t,
    part,
    up_ref,
    down_ref,
    up_far,
    down_far,
    xs,
    ps,
    scaled,
    pair_in,
    y_sum,
    y_in,
    mid,
    fin,
    x_in,
    z3_in,
    z4_in,
    z_in,
    load_sem,
    state_sem,
    send_sem,
    recv_sem,
):
    x, y, c = lax.axis_index("x"), lax.axis_index("y"), lax.axis_index("c")
    tp = 2 * y + c
    both = (1, -1)
    mate = {"x": lax.rem(x + 1 + 2 * lax.rem(x + c, 2), 4)}
    peers = [{"y": lax.rem(y + dy, 4), "c": lax.rem(c + dc, 2)} for dy in range(4) for dc in range(2) if dy or dc]
    ring = [neighbour("z", step) for step in (1, -1, 2, -2)] + [mate, neighbour("x", 2)]
    barrier = greet(peers + ring)

    heads, size = states.shape[0], states.shape[1]
    chunk = 16
    spans = [(h, slice(k, k + chunk)) for h in range(heads) for k in range(0, size, chunk)]
    load_tok = pltpu.make_async_copy(tok_hbm, blocks.at[tp], load_sem.at[0])
    load_up = pltpu.make_async_copy(up_hbm, up_ref, load_sem.at[1])
    load_down = pltpu.make_async_copy(down_hbm, down_ref, load_sem.at[2])
    load_w = []
    for i, w in enumerate((wq_hbm, wk_hbm, wv_hbm, wg_hbm)):
        load_w.append(pltpu.make_async_copy(w, w_ref.at[:, 128 * i : 128 * (i + 1)], load_sem.at[3 + i]))
    load_out = pltpu.make_async_copy(wo_hbm, wo_ref, load_sem.at[7])
    load_states = []
    for i, (h, k) in enumerate(spans):
        load_states.append(pltpu.make_async_copy(states_hbm.at[h, k], states.at[h, k], state_sem.at[i]))
    small = ((mix_gain_hbm, mix_gain_ref), (head_gain_hbm, head_gain_ref), (channel_gain_hbm, channel_gain_ref), (turn_hbm, turn_ref))
    load_small = [pltpu.make_async_copy(src, dst, load_sem.at[8 + i]) for i, (src, dst) in enumerate(small)]
    for copy in [load_tok, load_up, load_down] + load_small + load_w + load_states + [load_out]:
        copy.start()
    load_tok.wait()
    pl.semaphore_wait(barrier, len(peers) + len(ring))

    copies = Copies(send_sem, recv_sem)
    send = copies.send

    own = blocks.at[tp]
    near = {step: send(own, own, "y", step) for step in (2, 1, -1)}
    across = [send(own, own, "c", 1)]

    load_up.wait()
    load_down.wait()
    weights = []
    for held, far in ((up_ref, up_far), (down_ref, down_far)):
        deep = held.shape[0] // 4
        for i in range(2):
            rows = pl.ds(pl.multiple_of((2 * c + i) * deep, deep), deep)
            weights.append((far.at[rows], send(held.at[rows], far.at[rows], "x", 2)))
    handed = []

    def hand_over(i):
        there, copy = weights[i]
        copy.wait_recv()
        handed.append(send(there, there, "c", 1))

    for step in (1, -1, 2):
        near[step].wait_recv()
        arrived = blocks.at[2 * lax.rem(y + (4 - step), 4) + c]
        across.append(send(arrived, arrived, "c", 1))
    for copy in across:
        copy.wait_recv()

    for copy in load_small:
        copy.wait()
    width = blocks.shape[2]
    lanes = 128
    mix_gain = mix_gain_ref[...].astype(F32)
    total = 0.0
    for i in range(8):
        block = blocks[i].astype(F32)
        total = total + jnp.sum(block * block, axis=1, keepdims=True)
    inverse_rms = lax.rsqrt(total / D + EPSILON)
    for i in range(D // lanes):
        off = i * lanes % width
        block = blocks[i * lanes // width, :, off : off + lanes].astype(F32)
        normed[:, i * lanes : (i + 1) * lanes] = (block * inverse_rms * mix_gain[i : i + 1]).astype(BF16)
    for copy in load_w:
        copy.wait()
    projected = jnp.dot(normed[...], w_ref[...], preferred_element_type=F32)

    turned = [projected[:, 128 * i : 128 * (i + 1)].T for i in range(4)]
    cosine, sines = turn_ref[0 : size // 2], turn_ref[size // 2 : size]
    for source, target, scale in ((turned[0], q_t, size ** (-0.5)), (turned[1], k_t, 1.0)):
        for h in range(heads):
            first = source[h * size : h * size + size // 2]
            second = source[h * size + size // 2 : (h + 1) * size]
            target[h * size : h * size + size // 2] = (first * cosine - second * sines) * scale
            target[h * size + size // 2 : (h + 1) * size] = (first * sines + second * cosine) * scale
    for h in range(heads):
        head = jnp.full((1, lanes), heads * tp + h).astype(F32)
        decay = 1.0 - jnp.exp2(-1.0 - 11.0 * head / (HEADS - 1))
        rows = slice(h * size, (h + 1) * size)
        values = turned[2][rows]
        output = jnp.zeros_like(values)
        for i, (span_head, ks) in enumerate(spans):
            if span_head != h:
                continue
            load_states[i].wait()

            def step(j, output):
                for u in range(4):
                    k = ks.start + 4 * j + u
                    row = h * size + k
                    new = decay * states[h, k] + k_t[pl.ds(row, 1)] * values
                    new_ref[h, k] = new
                    output = output + q_t[pl.ds(row, 1)] * new
                return output

            output = lax.fori_loop(0, chunk // 4, step, output)
        center = output - jnp.mean(output, axis=0, keepdims=True)
        spread = jnp.mean(center * center, axis=0, keepdims=True)
        gate = turned[3][rows]
        gated_t[rows] = center * lax.rsqrt(spread + EPSILON) * (gate * jax.nn.sigmoid(gate))
    gated = (gated_t[...].T * head_gain_ref[...].astype(F32)).astype(BF16)
    load_out.wait()
    part[...] = jnp.dot(gated, wo_ref[...], preferred_element_type=F32).astype(BF16).reshape(8, 16, D)

    def rows_for(offset, core):
        return 2 * lax.rem(y + (offset + 4), 4) + core

    offsets = (2, 1, -1, 0)
    across = [send(part.at[rows_for(o, 1 - c)], pair_in.at[i], "c", 1) for i, o in enumerate(offsets)]

    def pair_sum(i):
        across[i].wait_recv()
        return part[rows_for(offsets[i], c)].astype(F32) + pair_in[i].astype(F32)

    near = []
    for i in range(3):
        y_sum[i] = pair_sum(i).astype(BF16)
        near.append(send(y_sum.at[i], y_in.at[i], "y", offsets[i]))
    attended = pair_sum(3)
    hand_over(0)
    mine = pl.ds(pl.multiple_of(16 * tp, 16), 16)
    own_rows = jnp.concatenate([blocks[i, mine] for i in range(8)], axis=1).astype(F32)
    for i in (1, 2, 0):
        near[i].wait_recv()
        attended = attended + y_in[i].astype(F32)
    middle = (own_rows + attended).astype(BF16)
    xs[0, 0] = middle
    mid[...] = middle

    z1, z2, z3, z4, xn = {}, {}, {}, {}, {}

    def to_mate(s):
        xn[s] = copies.send_to(xs.at[s, 0], xs.at[s, 1], mate)

    def halves(s):
        return (0, 1) if s > 0 else (1, 0)

    def side(h):
        return slice(h * D // 2, (h + 1) * D // 2)

    for i in range(2):
        for s in both:
            cols = side(halves(s)[i])
            z2[s, i] = send(xs.at[0, 0, :, cols], xs.at[slot(-2 * s), 0, :, cols], "z", 2 * s)
    for s in both:
        z1[s] = send(xs.at[0, 0], xs.at[slot(-s), 0], "z", s)
    to_mate(0)
    hand_over(1)
    for i in range(2):
        for s in both:
            z2[s, i].wait_recv()
            came = slot(-2 * s)
            cols = side(halves(s)[i])
            if i == 0:
                z4[s] = send(xs.at[came, 0, :, cols], xs.at[7, 0, :, cols], "z", 2 * s)
            z3[s, i] = send(xs.at[came, 0, :, cols], xs.at[slot(-3 * s), 0, :, cols], "z", s)
            if i == 1:
                to_mate(came)
    for s in both:
        z1[s].wait_recv()
        to_mate(slot(-s))
    for s in both:
        z4[s].wait_recv()
    to_mate(7)
    for s in both:
        for i in range(2):
            z3[s, i].wait_recv()
        to_mate(slot(-3 * s))
    hand_over(2)
    hand_over(3)

    gain = channel_gain_ref[...].astype(F32)

    def mix(first, stop):
        n = (stop - first) * 32
        squares = 0.0
        for i in range(D // lanes):
            cols = slice(i * lanes, (i + 1) * lanes)
            rows = xs[first:stop, :, :, cols].reshape(n, lanes).astype(F32)
            squares = squares + rows * rows
            scaled[0:n, cols] = (rows * gain[i : i + 1]).astype(BF16)
        second_rms = lax.rsqrt(jnp.sum(squares, axis=1, keepdims=True) / D + EPSILON)
        result = 0.0
        for up, down in ((up_ref, down_ref), (up_far, down_far)):
            hidden = jnp.dot(scaled[0:n], up[...], preferred_element_type=F32) * second_rms
            activated = jnp.square(jnp.maximum(hidden, 0.0)).astype(BF16)
            result = result + jnp.dot(activated, down[...], preferred_element_type=F32)
        ps[first:stop] = result.astype(BF16).reshape(stop - first, 2, 16, D)

    for copy in handed:
        copy.wait_recv()
    for s in range(5):
        xn[s].wait_recv()
    mix(0, 5)

    xo = {}

    def back_to_mate(s):
        xo[s] = copies.send_to(ps.at[s, 1], x_in.at[s], mate)

    def with_mate(s):
        xo[s].wait_recv()
        return ps[s, 0].astype(F32) + x_in[s].astype(F32)

    for s in (3, 4, 1, 2, 0):
        back_to_mate(s)
    for s in (7, 5, 6):
        xn[s].wait_recv()
    mix(5, 8)
    for s in (7, 5, 6):
        back_to_mate(s)

    o1, o2, o3, o4 = {}, {}, {}, {}
    ps[7, 0] = with_mate(7).astype(BF16)
    for s in both:
        cols = side(halves(s)[0])
        o4[s] = send(ps.at[7, 0, :, cols], z4_in.at[slot(s) - 1], "z", 2 * s)
    for s in both:
        ps[slot(3 * s), 0] = with_mate(slot(3 * s)).astype(BF16)
    for i in range(2):
        for s in both:
            cols = side(halves(s)[i])
            o3[s, i] = send(ps.at[slot(3 * s), 0, :, cols], z3_in.at[slot(s) - 1, :, cols], "z", s)
    for s in both:
        ps[slot(s), 0] = with_mate(slot(s)).astype(BF16)
        o1[s] = send(ps.at[slot(s), 0], z_in.at[slot(s) - 1], "z", s)
    relayed = {s: with_mate(slot(2 * s)) for s in both}
    for i in range(2):
        for s in both:
            there, cols = slot(2 * s), side(halves(s)[i])
            if i == 0:
                o4[s].wait_recv()
            o3[s, i].wait_recv()
            total = relayed[s][:, cols] + z3_in[slot(s) - 1, :, cols].astype(F32)
            if i == 0:
                total = total + z4_in[slot(s) - 1].astype(F32)
            ps[there, 0, :, cols] = total.astype(BF16)
            o2[s, i] = send(ps.at[there, 0, :, cols], z_in.at[slot(s) + 1, :, cols], "z", 2 * s)
    down_sum = with_mate(0) + mid[...].astype(F32)
    for s in both:
        o1[s].wait_recv()
        down_sum = down_sum + z_in[slot(s) - 1].astype(F32)
    for s in both:
        for i in range(2):
            o2[s, i].wait_recv()
        down_sum = down_sum + z_in[slot(s) + 1].astype(F32)
    fin[...] = down_sum.astype(BF16)

    def features(index):
        return pl.ds(pl.multiple_of(index * width, width), width)

    back = []
    for peer in peers:
        other = 2 * peer["y"] + peer["c"]
        back.append(copies.send_to(fin.at[:, features(other)], out_ref.at[tp], peer))
    out_ref[tp] = fin[:, features(tp)]
    for copy in back:
        copy.wait_recv()
    copies.finish()


def write_kernel(out_vmem, new_vmem, out_hbm, new_hbm, sem):
    copies = [pltpu.make_async_copy(out_vmem, out_hbm, sem.at[0])]
    heads, size = new_vmem.shape[0], new_vmem.shape[1]
    parts = 4
    for h in range(heads):
        for i in range(parts):
            k = slice(i * size // parts, (i + 1) * size // parts)
            copies.append(pltpu.make_async_copy(new_vmem.at[h, k], new_hbm.at[h, k], sem.at[len(copies)]))
    for copy in copies:
        copy.start()
    for copy in copies:
        copy.wait()


def write_out(out, new_states):
    vmem = pl.BlockSpec(memory_space=pltpu.VMEM)
    hbm = pl.BlockSpec(memory_space=pltpu.HBM)
    return pl.pallas_call(
        write_kernel,
        out_shape=(pltpu.HBM(out.shape, out.dtype), pltpu.HBM(new_states.shape, new_states.dtype)),
        in_specs=[vmem, vmem],
        out_specs=(hbm, hbm),
        scratch_shapes=[pltpu.SemaphoreType.DMA((9,))],
        compiler_params=pltpu.CompilerParams(vmem_limit_bytes=8 * 2**20),
        name="write_out",
    )(
        pltpu.with_memory_space_constraint(out, pltpu.VMEM),
        pltpu.with_memory_space_constraint(new_states, pltpu.VMEM),
    )


def in_hbm(array):
    return pltpu.with_memory_space_constraint(array, pltpu.HBM)


def local(
    tokens,
    states,
    mix_gain,
    w_query,
    w_key,
    w_value,
    w_gate,
    head_gain,
    w_output,
    channel_gain,
    w_up,
    w_down,
):
    rows, heads, size, _ = states.shape
    hidden = w_up.shape[1]
    angles = POS * ROTARY_BASE ** (-np.arange(size // 2) / (size // 2))
    turn = np.concatenate([np.cos(angles), np.sin(angles)]).astype(np.float32)[:, None]
    vmem = pl.BlockSpec(memory_space=pltpu.VMEM)
    hbm = pl.BlockSpec(memory_space=pltpu.HBM)
    copies = 80
    out, new_states = pl.pallas_call(
        layer_kernel,
        out_shape=(
            pltpu.VMEM((8, 16, tokens.shape[1]), BF16),
            pltpu.VMEM((heads, size, size, rows), F32),
        ),
        in_specs=[hbm] * 13,
        out_specs=(vmem, vmem),
        scratch_shapes=[
            pltpu.VMEM((D // 128, 128), BF16),
            pltpu.VMEM((1, heads * size), BF16),
            pltpu.VMEM((D // 128, 128), BF16),
            pltpu.VMEM((size, 1), F32),
            pltpu.VMEM((8, rows, tokens.shape[1]), BF16),
            pltpu.VMEM((D, 4 * heads * size), BF16),
            pltpu.VMEM((heads * size, D), BF16),
            pltpu.VMEM((heads, size, size, rows), F32),
            pltpu.VMEM((rows, D), BF16),
            pltpu.VMEM((heads * size, rows), F32),
            pltpu.VMEM((heads * size, rows), F32),
            pltpu.VMEM((heads * size, rows), F32),
            pltpu.VMEM((8, 16, D), BF16),
            pltpu.VMEM((D, hidden), BF16),
            pltpu.VMEM((hidden, D), BF16),
            pltpu.VMEM((D, hidden), BF16),
            pltpu.VMEM((hidden, D), BF16),
            pltpu.VMEM((8, 2, 16, D), BF16),
            pltpu.VMEM((8, 2, 16, D), BF16),
            pltpu.VMEM((160, D), BF16),
            pltpu.VMEM((4, 16, D), BF16),
            pltpu.VMEM((3, 16, D), BF16),
            pltpu.VMEM((3, 16, D), BF16),
            pltpu.VMEM((16, D), BF16),
            pltpu.VMEM((16, D), BF16),
            pltpu.VMEM((8, 16, D), BF16),
            pltpu.VMEM((2, 16, D), BF16),
            pltpu.VMEM((2, 16, D // 2), BF16),
            pltpu.VMEM((4, 16, D), BF16),
            pltpu.SemaphoreType.DMA((12,)),
            pltpu.SemaphoreType.DMA((heads * size // 16,)),
            pltpu.SemaphoreType.DMA((copies,)),
            pltpu.SemaphoreType.DMA((copies,)),
        ],
        compiler_params=pltpu.CompilerParams(
            collective_id=0, has_side_effects=True, vmem_limit_bytes=40 * 2**20
        ),
        name="layer",
    )(
        in_hbm(tokens),
        in_hbm(states.transpose(1, 2, 3, 0)),
        in_hbm(mix_gain.reshape(D // 128, 128)),
        in_hbm(w_query),
        in_hbm(w_key),
        in_hbm(w_value),
        in_hbm(w_gate),
        in_hbm(head_gain.reshape(1, heads * size)),
        in_hbm(w_output),
        in_hbm(channel_gain.reshape(D // 128, 128)),
        in_hbm(w_up),
        in_hbm(w_down),
        in_hbm(jnp.asarray(turn)),
    )
    out, new_states = write_out(out, new_states)
    return (out.reshape(tokens.shape), new_states.transpose(3, 0, 1, 2))


def solution(mesh):
    torus = Mesh(mesh.devices.reshape(8, 4, 4, 2), ("z", "x", "y", "c"))
    in_specs = (
        P(KV, TP),
        P(KV, TP, None, None),
        P(),
        P(None, TP),
        P(None, TP),
        P(None, TP),
        P(None, TP),
        P(TP),
        P(TP, None),
        P(),
        P(None, KV),
        P(KV, None),
    )
    out_specs = (P(KV, TP), P(KV, TP, None, None))
    return jax.shard_map(local, mesh=torus, in_specs=in_specs, out_specs=out_specs, check_vma=False)
```

```python
import jax
import jax.numpy as jnp
import numpy as np
from jax import lax
from jax.experimental import pallas as pl
from jax.experimental.pallas import tpu as pltpu
from jax.sharding import Mesh
from jax.sharding import PartitionSpec as P

HEADS = 16
POS = 16384
KV = ("z", "x")
TP = ("y", "c")

EPSILON = 1e-06
ROTARY_BASE = 10000.0

D = 2048
SIZES = {"z": 8, "x": 4, "y": 4, "c": 2}
F32 = jnp.float32
BF16 = jnp.bfloat16


def slot(offset):
    return 2 * abs(offset) - (1 if offset > 0 else 0)


class Copies:
    def __init__(self, send_sem, recv_sem):
        self.send_sem, self.recv_sem, self.made = send_sem, recv_sem, []

    def send_to(self, src, dst, device):
        index = len(self.made)
        copy = pltpu.make_async_remote_copy(
            src_ref=src,
            dst_ref=dst,
            send_sem=self.send_sem.at[index],
            recv_sem=self.recv_sem.at[index],
            device_id=device,
            device_id_type=pl.DeviceIdType.MESH,
        )
        copy.start()
        self.made.append(copy)
        return copy

    def send(self, src, dst, axis, step):
        return self.send_to(src, dst, neighbour(axis, step))

    def finish(self):
        for copy in self.made:
            copy.wait_send()


def greet(peers):
    barrier = pltpu.get_barrier_semaphore()
    for peer in peers:
        pl.semaphore_signal(barrier, inc=1, device_id=peer, device_id_type=pl.DeviceIdType.MESH)
    return barrier


def neighbour(axis, step):
    n = SIZES[axis]
    return {axis: lax.rem(lax.axis_index(axis) + (step + n), n)}


def half(start, stop, step):
    middle = (start + stop) // 2
    return slice(start, middle) if step > 0 else slice(middle, stop)


def layer_kernel(
    tok_hbm,
    states_hbm,
    mix_gain_hbm,
    wq_hbm,
    wk_hbm,
    wv_hbm,
    wg_hbm,
    head_gain_hbm,
    wo_hbm,
    channel_gain_hbm,
    up_hbm,
    down_hbm,
    turn_hbm,
    out_ref,
    new_ref,
    mix_gain_ref,
    head_gain_ref,
    channel_gain_ref,
    turn_ref,
    blocks,
    w_ref,
    wo_ref,
    states,
    normed,
    q_t,
    k_t,
    gated_t,
    part,
    up_ref,
    down_ref,
    up_far,
    down_far,
    xs,
    ps,
    scaled,
    pair_in,
    y_sum,
    y_in,
    mid,
    x_in,
    z3_in,
    z4_in,
    gathered,
    load_sem,
    state_sem,
    send_sem,
    recv_sem,
):
    x, y, c = lax.axis_index("x"), lax.axis_index("y"), lax.axis_index("c")
    tp = 2 * y + c
    both = (1, -1)
    mate = {"x": lax.rem(x + 1 + 2 * lax.rem(x + c, 2), 4)}
    peers = [{"y": lax.rem(y + dy, 4), "c": lax.rem(c + dc, 2)} for dy in range(4) for dc in range(2) if dy or dc]
    ring = [neighbour("z", step) for step in (1, -1, 2, -2)] + [mate, neighbour("x", 2)]
    barrier = greet(peers + ring)

    heads, size = states.shape[0], states.shape[1]
    chunk = 16
    spans = [(h, slice(k, k + chunk)) for h in range(heads) for k in range(0, size, chunk)]
    load_tok = pltpu.make_async_copy(tok_hbm, blocks.at[tp], load_sem.at[0])
    load_up = pltpu.make_async_copy(up_hbm, up_ref, load_sem.at[1])
    load_down = pltpu.make_async_copy(down_hbm, down_ref, load_sem.at[2])
    load_w = []
    for i, w in enumerate((wq_hbm, wk_hbm, wv_hbm, wg_hbm)):
        load_w.append(pltpu.make_async_copy(w, w_ref.at[:, 128 * i : 128 * (i + 1)], load_sem.at[3 + i]))
    load_out = pltpu.make_async_copy(wo_hbm, wo_ref, load_sem.at[7])
    load_states = []
    for i, (h, k) in enumerate(spans):
        load_states.append(pltpu.make_async_copy(states_hbm.at[h, k], states.at[h, k], state_sem.at[i]))
    small = ((mix_gain_hbm, mix_gain_ref), (head_gain_hbm, head_gain_ref), (channel_gain_hbm, channel_gain_ref), (turn_hbm, turn_ref))
    load_small = [pltpu.make_async_copy(src, dst, load_sem.at[8 + i]) for i, (src, dst) in enumerate(small)]
    for copy in [load_tok, load_up, load_down] + load_small + load_w + load_states + [load_out]:
        copy.start()
    load_tok.wait()
    pl.semaphore_wait(barrier, len(peers) + len(ring))

    copies = Copies(send_sem, recv_sem)
    send = copies.send

    own = blocks.at[tp]
    near = {step: send(own, own, "y", step) for step in (2, 1, -1)}
    across = [send(own, own, "c", 1)]

    load_up.wait()
    load_down.wait()
    eighth = down_ref.shape[0] // 8

    def down_rows(step, core):
        block = 2 * lax.rem(y + (4 - step), 4) + core
        return down_far.at[pl.ds(pl.multiple_of(block * eighth, eighth), eighth)]

    first_down = send(down_ref.at[pl.ds(pl.multiple_of(tp * eighth, eighth), eighth)], down_rows(0, c), "x", 2)
    weights = []
    deep = up_ref.shape[0] // 4
    for i in range(2):
        rows = pl.ds(pl.multiple_of((2 * c + i) * deep, deep), deep)
        weights.append((up_far.at[rows], send(up_ref.at[rows], up_far.at[rows], "x", 2)))
    handed = []

    def hand_over(i):
        there, copy = weights[i]
        copy.wait_recv()
        handed.append(send(there, there, "c", 1))

    for step in (1, -1, 2):
        near[step].wait_recv()
        arrived = blocks.at[2 * lax.rem(y + (4 - step), 4) + c]
        across.append(send(arrived, arrived, "c", 1))
    for copy in across:
        copy.wait_recv()

    for copy in load_small:
        copy.wait()
    width = blocks.shape[2]
    lanes = 128
    mix_gain = mix_gain_ref[...].astype(F32)
    total = 0.0
    for i in range(8):
        block = blocks[i].astype(F32)
        total = total + jnp.sum(block * block, axis=1, keepdims=True)
    inverse_rms = lax.rsqrt(total / D + EPSILON)
    for i in range(D // lanes):
        off = i * lanes % width
        block = blocks[i * lanes // width, :, off : off + lanes].astype(F32)
        normed[:, i * lanes : (i + 1) * lanes] = (block * inverse_rms * mix_gain[i : i + 1]).astype(BF16)
    for copy in load_w:
        copy.wait()
    projected = jnp.dot(normed[...], w_ref[...], preferred_element_type=F32)

    turned = [projected[:, 128 * i : 128 * (i + 1)].T for i in range(4)]
    cosine, sines = turn_ref[0 : size // 2], turn_ref[size // 2 : size]
    for source, target, scale in ((turned[0], q_t, size ** (-0.5)), (turned[1], k_t, 1.0)):
        for h in range(heads):
            first = source[h * size : h * size + size // 2]
            second = source[h * size + size // 2 : (h + 1) * size]
            target[h * size : h * size + size // 2] = (first * cosine - second * sines) * scale
            target[h * size + size // 2 : (h + 1) * size] = (first * sines + second * cosine) * scale
    for h in range(heads):
        head = jnp.full((1, lanes), heads * tp + h).astype(F32)
        decay = 1.0 - jnp.exp2(-1.0 - 11.0 * head / (HEADS - 1))
        rows = slice(h * size, (h + 1) * size)
        values = turned[2][rows]
        output = jnp.zeros_like(values)
        for i, (span_head, ks) in enumerate(spans):
            if span_head != h:
                continue
            load_states[i].wait()

            def step(j, output):
                for u in range(4):
                    k = ks.start + 4 * j + u
                    row = h * size + k
                    new = decay * states[h, k] + k_t[pl.ds(row, 1)] * values
                    new_ref[h, k] = new
                    output = output + q_t[pl.ds(row, 1)] * new
                return output

            output = lax.fori_loop(0, chunk // 4, step, output)
        center = output - jnp.mean(output, axis=0, keepdims=True)
        spread = jnp.mean(center * center, axis=0, keepdims=True)
        gate = turned[3][rows]
        gated_t[rows] = center * lax.rsqrt(spread + EPSILON) * (gate * jax.nn.sigmoid(gate))
    gated = (gated_t[...].T * head_gain_ref[...].astype(F32)).astype(BF16)
    load_out.wait()
    part[...] = jnp.dot(gated, wo_ref[...], preferred_element_type=F32).astype(BF16).reshape(8, 16, D)

    def rows_for(offset, core):
        return 2 * lax.rem(y + (offset + 4), 4) + core

    def side(h):
        return slice(h * D // 2, (h + 1) * D // 2)

    offsets = (2, 1, -1, 0)
    across, near = {}, {}
    for h in range(2):
        for i, o in enumerate(offsets):
            across[i, h] = send(part.at[rows_for(o, 1 - c), :, side(h)], pair_in.at[i, :, side(h)], "c", 1)

    def pair_sum(i, h):
        across[i, h].wait_recv()
        return part[rows_for(offsets[i], c), :, side(h)].astype(F32) + pair_in[i, :, side(h)].astype(F32)

    for h in range(2):
        for i in range(3):
            y_sum[i, :, side(h)] = pair_sum(i, h).astype(BF16)
            near[i, h] = send(y_sum.at[i, :, side(h)], y_in.at[i, :, side(h)], "y", offsets[i])
    mine = pl.ds(pl.multiple_of(16 * tp, 16), 16)
    own_rows = jnp.concatenate([blocks[i, mine] for i in range(8)], axis=1).astype(F32)
    z1, z2, z3, z4, xn = {}, {}, {}, {}, {}
    both_halves = (0, 1)
    for h in both_halves:
        attended = pair_sum(3, h)
        for i in (1, 2, 0):
            near[i, h].wait_recv()
            attended = attended + y_in[i, :, side(h)].astype(F32)
        middle = (own_rows[:, side(h)] + attended).astype(BF16)
        xs[0, 0, :, side(h)] = middle
        mid[:, side(h)] = middle
        for s in both:
            z2[s, h] = send(xs.at[0, 0, :, side(h)], xs.at[slot(-2 * s), 0, :, side(h)], "z", 2 * s)

    def to_mate(s):
        xn[s] = copies.send_to(xs.at[s, 0], xs.at[s, 1], mate)

    def features(index):
        return pl.ds(pl.multiple_of(index * width, width), width)

    everyone = [{"y": lax.rem(y + dy, 4), "c": lax.rem(c + dc, 2)} for dy in (2, 1, 3, 0) for dc in (1, 0)]
    spread = []

    def spread_out(row_ref, place, step=0):
        for peer in everyone if step else everyone[:-1]:
            other = 2 * peer["y"] + peer["c"]
            device = dict(peer, **neighbour("z", step)) if step else peer
            spread.append(copies.send_to(row_ref.at[:, features(other)], gathered.at[place, tp], device))
        if not step:
            gathered[place, tp] = row_ref[:, features(tp)]

    def halves(s):
        return (0, 1) if s > 0 else (1, 0)

    for s in both:
        z1[s] = send(xs.at[0, 0], xs.at[slot(-s), 0], "z", s)
    to_mate(0)
    first_down.wait_recv()
    along = {step: send(down_rows(0, c), down_rows(0, c), "y", step) for step in (2, 1, -1)}
    handed.append(send(down_rows(0, c), down_rows(0, c), "c", 1))
    hand_over(0)
    for h in both_halves:
        for s in both:
            z2[s, h].wait_recv()
            came = slot(-2 * s)
            if h == halves(s)[0]:
                z4[s] = send(xs.at[came, 0, :, side(h)], xs.at[7, 0, :, side(h)], "z", 2 * s)
            z3[s, h] = send(xs.at[came, 0, :, side(h)], xs.at[slot(-3 * s), 0, :, side(h)], "z", s)
            if h == 1:
                to_mate(came)
    hand_over(1)
    spread_out(mid, 5)
    for s in both:
        z1[s].wait_recv()
        to_mate(slot(-s))
    for step in (2, 1, -1):
        along[step].wait_recv()
        handed.append(send(down_rows(step, c), down_rows(step, c), "c", 1))
    for s in both:
        z4[s].wait_recv()
    to_mate(7)
    for s in both:
        for i in range(2):
            z3[s, i].wait_recv()
        to_mate(slot(-3 * s))
    gain = channel_gain_ref[...].astype(F32)

    def mix(first, stop):
        n = (stop - first) * 32
        squares = 0.0
        for i in range(D // lanes):
            cols = slice(i * lanes, (i + 1) * lanes)
            rows = xs[first:stop, :, :, cols].reshape(n, lanes).astype(F32)
            squares = squares + rows * rows
            scaled[0:n, cols] = (rows * gain[i : i + 1]).astype(BF16)
        second_rms = lax.rsqrt(jnp.sum(squares, axis=1, keepdims=True) / D + EPSILON)
        result = 0.0
        for up, down in ((up_ref, down_ref), (up_far, down_far)):
            hidden = jnp.dot(scaled[0:n], up[...], preferred_element_type=F32) * second_rms
            activated = jnp.square(jnp.maximum(hidden, 0.0)).astype(BF16)
            result = result + jnp.dot(activated, down[...], preferred_element_type=F32)
        ps[first:stop] = result.astype(BF16).reshape(stop - first, 2, 16, D)

    for copy in handed:
        copy.wait_recv()
    for s in range(5):
        xn[s].wait_recv()
    mix(0, 5)

    xo = {}

    def back_to_mate(s):
        xo[s] = copies.send_to(ps.at[s, 1], x_in.at[s], mate)

    def with_mate(s):
        xo[s].wait_recv()
        return ps[s, 0].astype(F32) + x_in[s].astype(F32)

    for s in (3, 4):
        back_to_mate(s)
    for s in (7, 5, 6):
        xn[s].wait_recv()
    mix(5, 8)
    back_to_mate(7)
    third = {}
    for i in range(2):
        for s in both:
            at, cols = slot(3 * s), side(halves(s)[i])
            third[s, i] = copies.send_to(ps.at[at, 1, :, cols], x_in.at[at, :, cols], mate)
    for s in (1, 2, 0):
        back_to_mate(s)

    o3, o4 = {}, {}
    ps[7, 0] = with_mate(7).astype(BF16)
    for s in both:
        cols = side(halves(s)[0])
        o4[s] = send(ps.at[7, 0, :, cols], z4_in.at[slot(s) - 1], "z", 2 * s)
    for i in range(2):
        for s in both:
            at, cols = slot(3 * s), side(halves(s)[i])
            third[s, i].wait_recv()
            ps[at, 0, :, cols] = (ps[at, 0, :, cols].astype(F32) + x_in[at, :, cols].astype(F32)).astype(BF16)
            o3[s, i] = send(ps.at[slot(3 * s), 0, :, cols], z3_in.at[slot(s) - 1, :, cols], "z", s)
    for s in both:
        ps[slot(s), 0] = with_mate(slot(s)).astype(BF16)
        spread_out(ps.at[slot(s), 0], slot(s) - 1, s)
    ps[0, 0] = with_mate(0).astype(BF16)
    spread_out(ps.at[0, 0], 4)
    relayed = {s: with_mate(slot(2 * s)) for s in both}
    for i in range(2):
        for s in both:
            there, cols = slot(2 * s), side(halves(s)[i])
            if i == 0:
                o4[s].wait_recv()
            o3[s, i].wait_recv()
            total = relayed[s][:, cols] + z3_in[slot(s) - 1, :, cols].astype(F32)
            if i == 0:
                total = total + z4_in[slot(s) - 1].astype(F32)
            ps[there, 0, :, cols] = total.astype(BF16)
    for s in both:
        spread_out(ps.at[slot(2 * s), 0], slot(s) + 1, 2 * s)
    for copy in spread:
        copy.wait_recv()
    total = 0.0
    for place in range(6):
        total = total + gathered[place].astype(F32)
    out_ref[...] = total.astype(BF16)
    copies.finish()


def write_kernel(out_vmem, new_vmem, out_hbm, new_hbm, sem):
    copies = [pltpu.make_async_copy(out_vmem, out_hbm, sem.at[0])]
    heads, size = new_vmem.shape[0], new_vmem.shape[1]
    parts = 4
    for h in range(heads):
        for i in range(parts):
            k = slice(i * size // parts, (i + 1) * size // parts)
            copies.append(pltpu.make_async_copy(new_vmem.at[h, k], new_hbm.at[h, k], sem.at[len(copies)]))
    for copy in copies:
        copy.start()
    for copy in copies:
        copy.wait()


def write_out(out, new_states):
    vmem = pl.BlockSpec(memory_space=pltpu.VMEM)
    hbm = pl.BlockSpec(memory_space=pltpu.HBM)
    return pl.pallas_call(
        write_kernel,
        out_shape=(pltpu.HBM(out.shape, out.dtype), pltpu.HBM(new_states.shape, new_states.dtype)),
        in_specs=[vmem, vmem],
        out_specs=(hbm, hbm),
        scratch_shapes=[pltpu.SemaphoreType.DMA((9,))],
        compiler_params=pltpu.CompilerParams(vmem_limit_bytes=8 * 2**20),
        name="write_out",
    )(
        pltpu.with_memory_space_constraint(out, pltpu.VMEM),
        pltpu.with_memory_space_constraint(new_states, pltpu.VMEM),
    )


def in_hbm(array):
    return pltpu.with_memory_space_constraint(array, pltpu.HBM)


def local(
    tokens,
    states,
    mix_gain,
    w_query,
    w_key,
    w_value,
    w_gate,
    head_gain,
    w_output,
    channel_gain,
    w_up,
    w_down,
):
    rows, heads, size, _ = states.shape
    hidden = w_up.shape[1]
    angles = POS * ROTARY_BASE ** (-np.arange(size // 2) / (size // 2))
    turn = np.concatenate([np.cos(angles), np.sin(angles)]).astype(np.float32)[:, None]
    vmem = pl.BlockSpec(memory_space=pltpu.VMEM)
    hbm = pl.BlockSpec(memory_space=pltpu.HBM)
    copies = 128
    out, new_states = pl.pallas_call(
        layer_kernel,
        out_shape=(
            pltpu.VMEM((8, 16, tokens.shape[1]), BF16),
            pltpu.VMEM((heads, size, size, rows), F32),
        ),
        in_specs=[hbm] * 13,
        out_specs=(vmem, vmem),
        scratch_shapes=[
            pltpu.VMEM((D // 128, 128), BF16),
            pltpu.VMEM((1, heads * size), BF16),
            pltpu.VMEM((D // 128, 128), BF16),
            pltpu.VMEM((size, 1), F32),
            pltpu.VMEM((8, rows, tokens.shape[1]), BF16),
            pltpu.VMEM((D, 4 * heads * size), BF16),
            pltpu.VMEM((heads * size, D), BF16),
            pltpu.VMEM((heads, size, size, rows), F32),
            pltpu.VMEM((rows, D), BF16),
            pltpu.VMEM((heads * size, rows), F32),
            pltpu.VMEM((heads * size, rows), F32),
            pltpu.VMEM((heads * size, rows), F32),
            pltpu.VMEM((8, 16, D), BF16),
            pltpu.VMEM((D, hidden), BF16),
            pltpu.VMEM((hidden, D), BF16),
            pltpu.VMEM((D, hidden), BF16),
            pltpu.VMEM((hidden, D), BF16),
            pltpu.VMEM((8, 2, 16, D), BF16),
            pltpu.VMEM((8, 2, 16, D), BF16),
            pltpu.VMEM((160, D), BF16),
            pltpu.VMEM((4, 16, D), BF16),
            pltpu.VMEM((3, 16, D), BF16),
            pltpu.VMEM((3, 16, D), BF16),
            pltpu.VMEM((16, D), BF16),
            pltpu.VMEM((8, 16, D), BF16),
            pltpu.VMEM((2, 16, D), BF16),
            pltpu.VMEM((2, 16, D // 2), BF16),
            pltpu.VMEM((6, 8, 16, tokens.shape[1]), BF16),
            pltpu.SemaphoreType.DMA((12,)),
            pltpu.SemaphoreType.DMA((heads * size // 16,)),
            pltpu.SemaphoreType.DMA((copies,)),
            pltpu.SemaphoreType.DMA((copies,)),
        ],
        compiler_params=pltpu.CompilerParams(
            collective_id=0, has_side_effects=True, vmem_limit_bytes=40 * 2**20
        ),
        name="layer",
    )(
        in_hbm(tokens),
        in_hbm(states.transpose(1, 2, 3, 0)),
        in_hbm(mix_gain.reshape(D // 128, 128)),
        in_hbm(w_query),
        in_hbm(w_key),
        in_hbm(w_value),
        in_hbm(w_gate),
        in_hbm(head_gain.reshape(1, heads * size)),
        in_hbm(w_output),
        in_hbm(channel_gain.reshape(D // 128, 128)),
        in_hbm(w_up),
        in_hbm(w_down),
        in_hbm(jnp.asarray(turn)),
    )
    out, new_states = write_out(out, new_states)
    return (out.reshape(tokens.shape), new_states.transpose(3, 0, 1, 2))


def solution(mesh):
    torus = Mesh(mesh.devices.reshape(8, 4, 4, 2), ("z", "x", "y", "c"))
    in_specs = (
        P(KV, TP),
        P(KV, TP, None, None),
        P(),
        P(None, TP),
        P(None, TP),
        P(None, TP),
        P(None, TP),
        P(TP),
        P(TP, None),
        P(),
        P(None, KV),
        P(KV, None),
    )
    out_specs = (P(KV, TP), P(KV, TP, None, None))
    return jax.shard_map(local, mesh=torus, in_specs=in_specs, out_specs=out_specs, check_vma=False)
```

```python
import jax
import jax.numpy as jnp
import numpy as np
from jax import lax
from jax.experimental import pallas as pl
from jax.experimental.pallas import tpu as pltpu
from jax.sharding import Mesh
from jax.sharding import PartitionSpec as P

HEADS = 16
POS = 16384
KV = ("z", "x")
TP = ("y", "c")

EPSILON = 1e-06
ROTARY_BASE = 10000.0

D = 2048
SIZES = {"z": 8, "x": 4, "y": 4, "c": 2}
F32 = jnp.float32
BF16 = jnp.bfloat16


def slot(offset):
    return 2 * abs(offset) - (1 if offset > 0 else 0)


class Copies:
    def __init__(self, send_sem, recv_sem):
        self.send_sem, self.recv_sem, self.made = send_sem, recv_sem, []

    def send_to(self, src, dst, device):
        index = len(self.made)
        copy = pltpu.make_async_remote_copy(
            src_ref=src,
            dst_ref=dst,
            send_sem=self.send_sem.at[index],
            recv_sem=self.recv_sem.at[index],
            device_id=device,
            device_id_type=pl.DeviceIdType.MESH,
        )
        copy.start()
        self.made.append(copy)
        return copy

    def send(self, src, dst, axis, step):
        return self.send_to(src, dst, neighbour(axis, step))

    def finish(self):
        for copy in self.made:
            copy.wait_send()


def greet(peers):
    barrier = pltpu.get_barrier_semaphore()
    for peer in peers:
        pl.semaphore_signal(barrier, inc=1, device_id=peer, device_id_type=pl.DeviceIdType.MESH)
    return barrier


def neighbour(axis, step):
    n = SIZES[axis]
    return {axis: lax.rem(lax.axis_index(axis) + (step + n), n)}


def half(start, stop, step):
    middle = (start + stop) // 2
    return slice(start, middle) if step > 0 else slice(middle, stop)


def layer_kernel(
    tok_hbm,
    states_hbm,
    mix_gain_hbm,
    wq_hbm,
    wk_hbm,
    wv_hbm,
    wg_hbm,
    head_gain_hbm,
    wo_hbm,
    channel_gain_hbm,
    up_hbm,
    down_hbm,
    turn_hbm,
    out_ref,
    new_ref,
    mix_gain_ref,
    head_gain_ref,
    channel_gain_ref,
    turn_ref,
    blocks,
    w_ref,
    wo_ref,
    states,
    projected,
    gain_rows,
    q_t,
    k_t,
    v_t,
    gated_t,
    gated_rows,
    gated_in,
    wo_pair,
    part,
    up_ref,
    down_ref,
    up_far,
    down_far,
    xs,
    ps,
    scaled,
    y_in,
    mid,
    x_in,
    z3_in,
    z4_in,
    gathered,
    load_sem,
    state_sem,
    send_sem,
    recv_sem,
):
    x, y, c = lax.axis_index("x"), lax.axis_index("y"), lax.axis_index("c")
    tp = 2 * y + c
    both = (1, -1)
    mate = {"x": lax.rem(x + 1 + 2 * lax.rem(x + c, 2), 4)}
    peers = [{"y": lax.rem(y + dy, 4), "c": lax.rem(c + dc, 2)} for dy in range(4) for dc in range(2) if dy or dc]
    ring = [neighbour("z", step) for step in (1, -1, 2, -2)] + [mate, neighbour("x", 2)]
    barrier = greet(peers + ring)

    heads, size = states.shape[0], states.shape[1]
    chunk = 16
    spans = [(h, slice(k, k + chunk)) for h in range(heads) for k in range(0, size, chunk)]
    load_tok = pltpu.make_async_copy(tok_hbm, blocks.at[tp], load_sem.at[0])
    load_up = pltpu.make_async_copy(up_hbm, up_ref, load_sem.at[1])
    load_down = pltpu.make_async_copy(down_hbm, down_ref, load_sem.at[2])
    load_w = []
    for i, w in enumerate((wq_hbm, wk_hbm, wv_hbm, wg_hbm)):
        load_w.append(pltpu.make_async_copy(w, w_ref.at[:, 128 * i : 128 * (i + 1)], load_sem.at[3 + i]))
    load_out = pltpu.make_async_copy(wo_hbm, wo_ref, load_sem.at[7])
    load_states = []
    for i, (h, k) in enumerate(spans):
        load_states.append(pltpu.make_async_copy(states_hbm.at[h, k], states.at[h, k], state_sem.at[i]))
    small = ((mix_gain_hbm, mix_gain_ref), (head_gain_hbm, head_gain_ref), (channel_gain_hbm, channel_gain_ref), (turn_hbm, turn_ref))
    load_small = [pltpu.make_async_copy(src, dst, load_sem.at[8 + i]) for i, (src, dst) in enumerate(small)]
    for copy in [load_tok, load_up, load_down] + load_small + load_w + load_states + [load_out]:
        copy.start()
    load_tok.wait()
    pl.semaphore_wait(barrier, len(peers) + len(ring))

    copies = Copies(send_sem, recv_sem)
    send = copies.send

    own = blocks.at[tp]
    near = {step: send(own, own, "y", step) for step in (2, 1, -1)}
    across = [send(own, own, "c", 1)]

    load_up.wait()
    load_down.wait()
    eighth = down_ref.shape[0] // 8

    def down_rows(step, core):
        block = 2 * lax.rem(y + (4 - step), 4) + core
        return down_far.at[pl.ds(pl.multiple_of(block * eighth, eighth), eighth)]

    first_down = send(down_ref.at[pl.ds(pl.multiple_of(tp * eighth, eighth), eighth)], down_rows(0, c), "x", 2)
    weights = []
    deep = up_ref.shape[0] // 4
    for i in range(2):
        rows = pl.ds(pl.multiple_of((2 * c + i) * deep, deep), deep)
        weights.append((up_far.at[rows], send(up_ref.at[rows], up_far.at[rows], "x", 2)))
    load_out.wait()
    pair_out = send(wo_ref, wo_pair, "c", 1)
    handed = []

    def hand_over(i):
        there, copy = weights[i]
        copy.wait_recv()
        handed.append(send(there, there, "c", 1))

    width = blocks.shape[2]
    lanes = 128
    for copy in load_small + load_w:
        copy.wait()
    gain_rows[...] = mix_gain_ref[...].astype(F32)

    def project(index, squares):
        block = blocks[index].astype(F32)
        gains = [gain_rows[pl.ds(index * (width // lanes) + i, 1)] for i in range(width // lanes)]
        scaled_block = (block * jnp.concatenate(gains, axis=1)).astype(BF16)
        rows = pl.ds(pl.multiple_of(index * width, width), width)
        product = jnp.dot(scaled_block, w_ref[rows], preferred_element_type=F32)
        if squares is None:
            projected[...] = product
            return jnp.sum(block * block, axis=1, keepdims=True)
        projected[...] += product
        return squares + jnp.sum(block * block, axis=1, keepdims=True)

    def block_of(step, core):
        return 2 * lax.rem(y + (4 - step), 4) + core

    total = project(tp, None)
    for step in (1, -1, 2):
        near[step].wait_recv()
        arrived = blocks.at[block_of(step, c)]
        across.append(send(arrived, arrived, "c", 1))
    for step in (1, -1, 2):
        total = project(block_of(step, c), total)
    for i, step in enumerate((0, 1, -1, 2)):
        across[i].wait_recv()
        total = project(block_of(step, 1 - c), total)
    inverse_rms = lax.rsqrt(total / D + EPSILON)

    turned = [(projected[:, 128 * i : 128 * (i + 1)] * inverse_rms).T for i in range(4)]
    cosine, sines = turn_ref[0 : size // 2], turn_ref[size // 2 : size]
    for source, target, scale in ((turned[0], q_t, size ** (-0.5)), (turned[1], k_t, 1.0)):
        for h in range(heads):
            first = source[h * size : h * size + size // 2]
            second = source[h * size + size // 2 : (h + 1) * size]
            target[h * size : h * size + size // 2] = (first * cosine - second * sines) * scale
            target[h * size + size // 2 : (h + 1) * size] = (first * sines + second * cosine) * scale
    v_t[...] = turned[2]

    def decay_of(h):
        head = jnp.full((1, lanes), heads * tp + h).astype(F32)
        return 1.0 - jnp.exp2(-1.0 - 11.0 * head / (HEADS - 1))

    for h in range(heads):
        rows = slice(h * size, (h + 1) * size)
        values = turned[2][rows]
        sums = jnp.zeros_like(values)
        for i, (span_head, ks) in enumerate(spans):
            if span_head != h:
                continue
            load_states[i].wait()

            def step(j, sums):
                for u in range(8):
                    k = ks.start + 8 * j + u
                    sums = sums + q_t[pl.ds(h * size + k, 1)] * states[h, k]
                return sums

            sums = lax.fori_loop(0, chunk // 8, step, sums)
        overlap = jnp.sum(q_t[rows] * k_t[rows], axis=0, keepdims=True)
        output = decay_of(h) * sums + overlap * values
        center = output - jnp.mean(output, axis=0, keepdims=True)
        spread = jnp.mean(center * center, axis=0, keepdims=True)
        gate = turned[3][rows]
        gated_t[rows] = center * lax.rsqrt(spread + EPSILON) * (gate * jax.nn.sigmoid(gate))
    gated = (gated_t[...].T * head_gain_ref[...].astype(F32)).astype(BF16)
    gated_rows[...] = gated.reshape(4, 2, 16, heads * size)

    traded = send(gated_rows.at[:, 1 - c], gated_in, "c", 1)

    def side(h):
        return slice(h * D // 2, (h + 1) * D // 2)

    offsets = (2, 1, -1)
    near = {}
    own_gated = gated_rows[:, c].reshape(64, heads * size)
    firsts = [jnp.dot(own_gated, wo_ref[:, side(h)], preferred_element_type=F32) for h in range(2)]
    pair_out.wait_recv()
    traded.wait_recv()
    other_gated = gated_in[...].reshape(64, heads * size)
    for h in range(2):
        product = firsts[h] + jnp.dot(other_gated, wo_pair[:, side(h)], preferred_element_type=F32)
        part[:, :, side(h)] = product.astype(BF16).reshape(4, 16, D // 2)
        for i, o in enumerate(offsets):
            there = part.at[lax.rem(y + (o + 4), 4), :, side(h)]
            near[i, h] = send(there, y_in.at[i, :, side(h)], "y", o)
    mine = pl.ds(pl.multiple_of(16 * tp, 16), 16)
    own_rows = jnp.concatenate([blocks[i, mine] for i in range(8)], axis=1).astype(F32)
    z1, z2, z3, z4, xn = {}, {}, {}, {}, {}
    both_halves = (0, 1)
    for h in both_halves:
        attended = part[y, :, side(h)].astype(F32)
        for i in (1, 2, 0):
            near[i, h].wait_recv()
            attended = attended + y_in[i, :, side(h)].astype(F32)
        middle = (own_rows[:, side(h)] + attended).astype(BF16)
        xs[0, 0, :, side(h)] = middle
        mid[:, side(h)] = middle
        for s in both:
            z2[s, h] = send(xs.at[0, 0, :, side(h)], xs.at[slot(-2 * s), 0, :, side(h)], "z", 2 * s)

    def half_to_mate(s, h):
        xn[s, h] = copies.send_to(xs.at[s, 0, :, side(h)], xs.at[s, 1, :, side(h)], mate)

    def to_mate(s):
        xn[s] = copies.send_to(xs.at[s, 0], xs.at[s, 1], mate)

    def features(index):
        return pl.ds(pl.multiple_of(index * width, width), width)

    everyone = [{"y": lax.rem(y + dy, 4), "c": lax.rem(c + dc, 2)} for dy in (2, 1, 3, 0) for dc in (1, 0)]
    spread = []

    def spread_out(row_ref, place, step=0):
        for peer in everyone if step else everyone[:-1]:
            other = 2 * peer["y"] + peer["c"]
            device = dict(peer, **neighbour("z", step)) if step else peer
            spread.append(copies.send_to(row_ref.at[:, features(other)], gathered.at[place, tp], device))
        if not step:
            gathered[place, tp] = row_ref[:, features(tp)]

    def halves(s):
        return (0, 1) if s > 0 else (1, 0)

    for s in both:
        z1[s] = send(xs.at[0, 0], xs.at[slot(-s), 0], "z", s)
    to_mate(0)
    first_down.wait_recv()
    along = {step: send(down_rows(0, c), down_rows(0, c), "y", step) for step in (2, 1, -1)}
    handed.append(send(down_rows(0, c), down_rows(0, c), "c", 1))
    hand_over(0)
    for h in range(heads):
        decay = decay_of(h)
        values = v_t[h * size : (h + 1) * size]

        def renew(j, carry):
            for u in range(8):
                k = 8 * j + u
                new_ref[h, k] = decay * states[h, k] + k_t[pl.ds(h * size + k, 1)] * values
            return carry

        lax.fori_loop(0, size // 8, renew, 0)
    for h in both_halves:
        for s in both:
            z2[s, h].wait_recv()
            came = slot(-2 * s)
            if h == halves(s)[0]:
                z4[s] = send(xs.at[came, 0, :, side(h)], xs.at[7, 0, :, side(h)], "z", 2 * s)
            z3[s, h] = send(xs.at[came, 0, :, side(h)], xs.at[slot(-3 * s), 0, :, side(h)], "z", s)
            half_to_mate(came, h)
    hand_over(1)
    spread_out(mid, 5)
    for s in both:
        z1[s].wait_recv()
        to_mate(slot(-s))
    for step in (2, 1, -1):
        along[step].wait_recv()
        handed.append(send(down_rows(step, c), down_rows(step, c), "c", 1))
    for s in both:
        z4[s].wait_recv()
    to_mate(7)
    for s in both:
        z3[s, 0].wait_recv()
        half_to_mate(slot(-3 * s), 0)
    for s in both:
        z3[s, 1].wait_recv()
        half_to_mate(slot(-3 * s), 1)
    gain = channel_gain_ref[...].astype(F32)

    def mix(first, stop):
        n = (stop - first) * 32
        squares = 0.0
        for i in range(D // lanes):
            cols = slice(i * lanes, (i + 1) * lanes)
            rows = xs[first:stop, :, :, cols].reshape(n, lanes).astype(F32)
            squares = squares + rows * rows
            scaled[0:n, cols] = (rows * gain[i : i + 1]).astype(BF16)
        second_rms = lax.rsqrt(jnp.sum(squares, axis=1, keepdims=True) / D + EPSILON)
        result = 0.0
        for up, down in ((up_ref, down_ref), (up_far, down_far)):
            hidden = jnp.dot(scaled[0:n], up[...], preferred_element_type=F32) * second_rms
            activated = jnp.square(jnp.maximum(hidden, 0.0)).astype(BF16)
            result = result + jnp.dot(activated, down[...], preferred_element_type=F32)
        ps[first:stop] = result.astype(BF16).reshape(stop - first, 2, 16, D)

    for copy in handed:
        copy.wait_recv()
    for key in (0, (3, 0), (4, 0), (3, 1), (4, 1), 1, 2):
        xn[key].wait_recv()
    mix(0, 5)

    xo = {}

    def back_to_mate(s):
        xo[s] = copies.send_to(ps.at[s, 1], x_in.at[s], mate)

    def with_mate(s):
        xo[s].wait_recv()
        return ps[s, 0].astype(F32) + x_in[s].astype(F32)

    for s in (3, 4, 1):
        back_to_mate(s)
    for key in (7, (5, 0), (6, 0), (5, 1), (6, 1)):
        xn[key].wait_recv()
    mix(5, 8)
    back_to_mate(7)
    third = {}
    for i in range(2):
        for s in both:
            at, cols = slot(3 * s), side(halves(s)[i])
            third[s, i] = copies.send_to(ps.at[at, 1, :, cols], x_in.at[at, :, cols], mate)
    for s in (2, 0):
        back_to_mate(s)

    o3, o4 = {}, {}
    ps[7, 0] = with_mate(7).astype(BF16)
    for s in both:
        cols = side(halves(s)[0])
        o4[s] = send(ps.at[7, 0, :, cols], z4_in.at[slot(s) - 1], "z", 2 * s)
    for i in range(2):
        for s in both:
            at, cols = slot(3 * s), side(halves(s)[i])
            third[s, i].wait_recv()
            ps[at, 0, :, cols] = (ps[at, 0, :, cols].astype(F32) + x_in[at, :, cols].astype(F32)).astype(BF16)
            o3[s, i] = send(ps.at[slot(3 * s), 0, :, cols], z3_in.at[slot(s) - 1, :, cols], "z", s)
    for s in both:
        ps[slot(s), 0] = with_mate(slot(s)).astype(BF16)
        spread_out(ps.at[slot(s), 0], slot(s) - 1, s)
    ps[0, 0] = with_mate(0).astype(BF16)
    spread_out(ps.at[0, 0], 4)
    relayed = {s: with_mate(slot(2 * s)) for s in both}
    for i in range(2):
        for s in both:
            there, cols = slot(2 * s), side(halves(s)[i])
            if i == 0:
                o4[s].wait_recv()
            o3[s, i].wait_recv()
            total = relayed[s][:, cols] + z3_in[slot(s) - 1, :, cols].astype(F32)
            if i == 0:
                total = total + z4_in[slot(s) - 1].astype(F32)
            ps[there, 0, :, cols] = total.astype(BF16)
            if i == 1:
                spread_out(ps.at[there, 0], slot(s) + 1, 2 * s)
    for copy in spread:
        copy.wait_recv()
    total = 0.0
    for place in range(6):
        total = total + gathered[place].astype(F32)
    out_ref[...] = total.astype(BF16)
    copies.finish()


def write_kernel(out_vmem, new_vmem, out_hbm, new_hbm, sem):
    copies = [pltpu.make_async_copy(out_vmem, out_hbm, sem.at[0])]
    heads, size = new_vmem.shape[0], new_vmem.shape[1]
    parts = 4
    for h in range(heads):
        for i in range(parts):
            k = slice(i * size // parts, (i + 1) * size // parts)
            copies.append(pltpu.make_async_copy(new_vmem.at[h, k], new_hbm.at[h, k], sem.at[len(copies)]))
    for copy in copies:
        copy.start()
    for copy in copies:
        copy.wait()


def write_out(out, new_states):
    vmem = pl.BlockSpec(memory_space=pltpu.VMEM)
    hbm = pl.BlockSpec(memory_space=pltpu.HBM)
    return pl.pallas_call(
        write_kernel,
        out_shape=(pltpu.HBM(out.shape, out.dtype), pltpu.HBM(new_states.shape, new_states.dtype)),
        in_specs=[vmem, vmem],
        out_specs=(hbm, hbm),
        scratch_shapes=[pltpu.SemaphoreType.DMA((9,))],
        compiler_params=pltpu.CompilerParams(vmem_limit_bytes=8 * 2**20),
        name="write_out",
    )(
        pltpu.with_memory_space_constraint(out, pltpu.VMEM),
        pltpu.with_memory_space_constraint(new_states, pltpu.VMEM),
    )


def in_hbm(array):
    return pltpu.with_memory_space_constraint(array, pltpu.HBM)


def local(
    tokens,
    states,
    mix_gain,
    w_query,
    w_key,
    w_value,
    w_gate,
    head_gain,
    w_output,
    channel_gain,
    w_up,
    w_down,
):
    rows, heads, size, _ = states.shape
    hidden = w_up.shape[1]
    angles = POS * ROTARY_BASE ** (-np.arange(size // 2) / (size // 2))
    turn = np.concatenate([np.cos(angles), np.sin(angles)]).astype(np.float32)[:, None]
    vmem = pl.BlockSpec(memory_space=pltpu.VMEM)
    hbm = pl.BlockSpec(memory_space=pltpu.HBM)
    copies = 128
    out, new_states = pl.pallas_call(
        layer_kernel,
        out_shape=(
            pltpu.VMEM((8, 16, tokens.shape[1]), BF16),
            pltpu.VMEM((heads, size, size, rows), F32),
        ),
        in_specs=[hbm] * 13,
        out_specs=(vmem, vmem),
        scratch_shapes=[
            pltpu.VMEM((D // 128, 128), BF16),
            pltpu.VMEM((1, heads * size), BF16),
            pltpu.VMEM((D // 128, 128), BF16),
            pltpu.VMEM((size, 1), F32),
            pltpu.VMEM((8, rows, tokens.shape[1]), BF16),
            pltpu.VMEM((D, 4 * heads * size), BF16),
            pltpu.VMEM((heads * size, D), BF16),
            pltpu.VMEM((heads, size, size, rows), F32),
            pltpu.VMEM((rows, 4 * heads * size), F32),
            pltpu.VMEM((D // 128, 128), F32),
            pltpu.VMEM((heads * size, rows), F32),
            pltpu.VMEM((heads * size, rows), F32),
            pltpu.VMEM((heads * size, rows), F32),
            pltpu.VMEM((heads * size, rows), F32),
            pltpu.VMEM((4, 2, 16, heads * size), BF16),
            pltpu.VMEM((4, 16, heads * size), BF16),
            pltpu.VMEM((heads * size, D), BF16),
            pltpu.VMEM((4, 16, D), BF16),
            pltpu.VMEM((D, hidden), BF16),
            pltpu.VMEM((hidden, D), BF16),
            pltpu.VMEM((D, hidden), BF16),
            pltpu.VMEM((hidden, D), BF16),
            pltpu.VMEM((8, 2, 16, D), BF16),
            pltpu.VMEM((8, 2, 16, D), BF16),
            pltpu.VMEM((160, D), BF16),
            pltpu.VMEM((3, 16, D), BF16),
            pltpu.VMEM((16, D), BF16),
            pltpu.VMEM((8, 16, D), BF16),
            pltpu.VMEM((2, 16, D), BF16),
            pltpu.VMEM((2, 16, D // 2), BF16),
            pltpu.VMEM((6, 8, 16, tokens.shape[1]), BF16),
            pltpu.SemaphoreType.DMA((12,)),
            pltpu.SemaphoreType.DMA((heads * size // 16,)),
            pltpu.SemaphoreType.DMA((copies,)),
            pltpu.SemaphoreType.DMA((copies,)),
        ],
        compiler_params=pltpu.CompilerParams(
            collective_id=0, has_side_effects=True, vmem_limit_bytes=40 * 2**20
        ),
        name="layer",
    )(
        in_hbm(tokens),
        in_hbm(states.transpose(1, 2, 3, 0)),
        in_hbm(mix_gain.reshape(D // 128, 128)),
        in_hbm(w_query),
        in_hbm(w_key),
        in_hbm(w_value),
        in_hbm(w_gate),
        in_hbm(head_gain.reshape(1, heads * size)),
        in_hbm(w_output),
        in_hbm(channel_gain.reshape(D // 128, 128)),
        in_hbm(w_up),
        in_hbm(w_down),
        in_hbm(jnp.asarray(turn)),
    )
    out, new_states = write_out(out, new_states)
    return (out.reshape(tokens.shape), new_states.transpose(3, 0, 1, 2))


def solution(mesh):
    torus = Mesh(mesh.devices.reshape(8, 4, 4, 2), ("z", "x", "y", "c"))
    in_specs = (
        P(KV, TP),
        P(KV, TP, None, None),
        P(),
        P(None, TP),
        P(None, TP),
        P(None, TP),
        P(None, TP),
        P(TP),
        P(TP, None),
        P(),
        P(None, KV),
        P(KV, None),
    )
    out_specs = (P(KV, TP), P(KV, TP, None, None))
    return jax.shard_map(local, mesh=torus, in_specs=in_specs, out_specs=out_specs, check_vma=False)
```

```python
import jax
import jax.numpy as jnp
import numpy as np
from jax import lax
from jax.experimental import pallas as pl
from jax.experimental.pallas import tpu as pltpu
from jax.sharding import Mesh
from jax.sharding import PartitionSpec as P

HEADS = 16
POS = 16384
KV = ("z", "x")
TP = ("y", "c")

EPSILON = 1e-06
ROTARY_BASE = 10000.0

D = 2048
SIZES = {"z": 8, "x": 4, "y": 4, "c": 2}
F32 = jnp.float32
BF16 = jnp.bfloat16


def slot(offset):
    return 2 * abs(offset) - (1 if offset > 0 else 0)


class Copies:
    def __init__(self, send_sem, recv_sem):
        self.send_sem, self.recv_sem, self.made = send_sem, recv_sem, []

    def send_to(self, src, dst, device):
        index = len(self.made)
        copy = pltpu.make_async_remote_copy(
            src_ref=src,
            dst_ref=dst,
            send_sem=self.send_sem.at[index],
            recv_sem=self.recv_sem.at[index],
            device_id=device,
            device_id_type=pl.DeviceIdType.MESH,
        )
        copy.start()
        self.made.append(copy)
        return copy

    def send(self, src, dst, axis, step):
        return self.send_to(src, dst, neighbour(axis, step))

    def finish(self):
        for copy in self.made:
            copy.wait_send()


def greet(peers):
    barrier = pltpu.get_barrier_semaphore()
    for peer in peers:
        pl.semaphore_signal(barrier, inc=1, device_id=peer, device_id_type=pl.DeviceIdType.MESH)
    return barrier


def neighbour(axis, step):
    n = SIZES[axis]
    return {axis: lax.rem(lax.axis_index(axis) + (step + n), n)}


def half(start, stop, step):
    middle = (start + stop) // 2
    return slice(start, middle) if step > 0 else slice(middle, stop)


def layer_kernel(
    tok_hbm,
    states_hbm,
    mix_gain_hbm,
    wq_hbm,
    wk_hbm,
    wv_hbm,
    wg_hbm,
    head_gain_hbm,
    wo_hbm,
    channel_gain_hbm,
    up_hbm,
    down_hbm,
    turn_hbm,
    out_ref,
    new_ref,
    mix_gain_ref,
    head_gain_ref,
    channel_gain_ref,
    turn_ref,
    blocks,
    w_ref,
    wo_ref,
    states,
    projected,
    gain_rows,
    q_t,
    k_t,
    v_t,
    gated_t,
    gated_rows,
    gated_in,
    wo_pair,
    part,
    up_ref,
    down_ref,
    up_far,
    down_far,
    xs,
    ps,
    scaled,
    y_in,
    mid,
    x_in,
    z3_in,
    z4_in,
    gathered,
    load_sem,
    state_sem,
    send_sem,
    recv_sem,
):
    x, y, c = lax.axis_index("x"), lax.axis_index("y"), lax.axis_index("c")
    tp = 2 * y + c
    both = (1, -1)
    mate = {"x": lax.rem(x + 1 + 2 * lax.rem(x + c, 2), 4)}
    peers = [{"y": lax.rem(y + dy, 4), "c": lax.rem(c + dc, 2)} for dy in range(4) for dc in range(2) if dy or dc]
    ring = [neighbour("z", step) for step in (1, -1, 2, -2)] + [mate, neighbour("x", 2)]
    barrier = greet(peers + ring)

    heads, size = states.shape[0], states.shape[1]
    chunk = 16
    spans = [(h, slice(k, k + chunk)) for h in range(heads) for k in range(0, size, chunk)]
    load_tok = pltpu.make_async_copy(tok_hbm, blocks.at[tp], load_sem.at[0])
    load_up = pltpu.make_async_copy(up_hbm, up_ref, load_sem.at[1])
    load_down = pltpu.make_async_copy(down_hbm, down_ref, load_sem.at[2])
    load_w = []
    for i, w in enumerate((wq_hbm, wk_hbm, wv_hbm, wg_hbm)):
        load_w.append(pltpu.make_async_copy(w, w_ref.at[:, 128 * i : 128 * (i + 1)], load_sem.at[3 + i]))
    load_out = pltpu.make_async_copy(wo_hbm, wo_ref, load_sem.at[7])
    load_states = []
    for i, (h, k) in enumerate(spans):
        load_states.append(pltpu.make_async_copy(states_hbm.at[h, k], states.at[h, k], state_sem.at[i]))
    small = ((mix_gain_hbm, mix_gain_ref), (head_gain_hbm, head_gain_ref), (channel_gain_hbm, channel_gain_ref), (turn_hbm, turn_ref))
    load_small = [pltpu.make_async_copy(src, dst, load_sem.at[8 + i]) for i, (src, dst) in enumerate(small)]
    for copy in [load_tok, load_up, load_down] + load_small + load_w + load_states + [load_out]:
        copy.start()
    load_tok.wait()
    pl.semaphore_wait(barrier, len(peers) + len(ring))

    copies = Copies(send_sem, recv_sem)
    send = copies.send

    own = blocks.at[tp]
    near = {step: send(own, own, "y", step) for step in (2, 1, -1)}
    across = [send(own, own, "c", 1)]

    load_up.wait()
    load_down.wait()
    eighth = down_ref.shape[0] // 8

    def down_rows(step, core):
        block = 2 * lax.rem(y + (4 - step), 4) + core
        return down_far.at[pl.ds(pl.multiple_of(block * eighth, eighth), eighth)]

    first_down = send(down_ref.at[pl.ds(pl.multiple_of(tp * eighth, eighth), eighth)], down_rows(0, c), "x", 2)
    weights = []
    deep = up_ref.shape[0] // 4
    for i in range(2):
        rows = pl.ds(pl.multiple_of((2 * c + i) * deep, deep), deep)
        weights.append((up_far.at[rows], send(up_ref.at[rows], up_far.at[rows], "x", 2)))
    load_out.wait()
    pair_out = send(wo_ref, wo_pair, "c", 1)
    handed = []

    def hand_over(i):
        there, copy = weights[i]
        copy.wait_recv()
        handed.append(send(there, there, "c", 1))

    width = blocks.shape[2]
    lanes = 128
    for copy in load_small + load_w:
        copy.wait()
    gain_rows[...] = mix_gain_ref[...].astype(F32)

    def project(index, squares):
        block = blocks[index].astype(F32)
        gains = [gain_rows[pl.ds(index * (width // lanes) + i, 1)] for i in range(width // lanes)]
        scaled_block = (block * jnp.concatenate(gains, axis=1)).astype(BF16)
        rows = pl.ds(pl.multiple_of(index * width, width), width)
        product = jnp.dot(scaled_block, w_ref[rows], preferred_element_type=F32)
        if squares is None:
            projected[...] = product
            return jnp.sum(block * block, axis=1, keepdims=True)
        projected[...] += product
        return squares + jnp.sum(block * block, axis=1, keepdims=True)

    def block_of(step, core):
        return 2 * lax.rem(y + (4 - step), 4) + core

    total = project(tp, None)
    for step in (1, -1, 2):
        near[step].wait_recv()
        arrived = blocks.at[block_of(step, c)]
        across.append(send(arrived, arrived, "c", 1))
    for step in (1, -1, 2):
        total = project(block_of(step, c), total)
    for i, step in enumerate((0, 1, -1, 2)):
        across[i].wait_recv()
        total = project(block_of(step, 1 - c), total)
    inverse_rms = lax.rsqrt(total / D + EPSILON)

    turned = [(projected[:, 128 * i : 128 * (i + 1)] * inverse_rms).T for i in range(4)]
    cosine, sines = turn_ref[0 : size // 2], turn_ref[size // 2 : size]
    for source, target, scale in ((turned[0], q_t, size ** (-0.5)), (turned[1], k_t, 1.0)):
        for h in range(heads):
            first = source[h * size : h * size + size // 2]
            second = source[h * size + size // 2 : (h + 1) * size]
            target[h * size : h * size + size // 2] = (first * cosine - second * sines) * scale
            target[h * size + size // 2 : (h + 1) * size] = (first * sines + second * cosine) * scale
    v_t[...] = turned[2]

    def decay_of(h):
        head = jnp.full((1, lanes), heads * tp + h).astype(F32)
        return 1.0 - jnp.exp2(-1.0 - 11.0 * head / (HEADS - 1))

    for h in range(heads):
        rows = slice(h * size, (h + 1) * size)
        values = turned[2][rows]
        sums = jnp.zeros_like(values)
        for i, (span_head, ks) in enumerate(spans):
            if span_head != h:
                continue
            load_states[i].wait()

            def step(j, sums):
                for u in range(8):
                    k = ks.start + 8 * j + u
                    sums = sums + q_t[pl.ds(h * size + k, 1)] * states[h, k]
                return sums

            sums = lax.fori_loop(0, chunk // 8, step, sums)
        overlap = jnp.sum(q_t[rows] * k_t[rows], axis=0, keepdims=True)
        output = decay_of(h) * sums + overlap * values
        center = output - jnp.mean(output, axis=0, keepdims=True)
        spread = jnp.mean(center * center, axis=0, keepdims=True)
        gate = turned[3][rows]
        gated_t[rows] = center * lax.rsqrt(spread + EPSILON) * (gate * jax.nn.sigmoid(gate))
    gated = (gated_t[...].T * head_gain_ref[...].astype(F32)).astype(BF16)
    gated_rows[...] = gated.reshape(4, 2, 16, heads * size)

    traded = send(gated_rows.at[:, 1 - c], gated_in, "c", 1)

    def side(h):
        return slice(h * D // 2, (h + 1) * D // 2)

    offsets = (2, 1, -1)
    near = {}
    own_gated = gated_rows[:, c].reshape(64, heads * size)
    firsts = [jnp.dot(own_gated, wo_ref[:, side(h)], preferred_element_type=F32) for h in range(2)]
    pair_out.wait_recv()
    traded.wait_recv()
    other_gated = gated_in[...].reshape(64, heads * size)
    for h in range(2):
        product = firsts[h] + jnp.dot(other_gated, wo_pair[:, side(h)], preferred_element_type=F32)
        part[:, :, side(h)] = product.astype(BF16).reshape(4, 16, D // 2)
        for i, o in enumerate(offsets):
            there = part.at[lax.rem(y + (o + 4), 4), :, side(h)]
            near[i, h] = send(there, y_in.at[i, :, side(h)], "y", o)
    mine = pl.ds(pl.multiple_of(16 * tp, 16), 16)
    own_rows = jnp.concatenate([blocks[i, mine] for i in range(8)], axis=1).astype(F32)
    z1, z2, z3, z4, xn = {}, {}, {}, {}, {}
    both_halves = (0, 1)
    for h in both_halves:
        attended = part[y, :, side(h)].astype(F32)
        for i in (1, 2, 0):
            near[i, h].wait_recv()
            attended = attended + y_in[i, :, side(h)].astype(F32)
        middle = (own_rows[:, side(h)] + attended).astype(BF16)
        xs[0, 0, :, side(h)] = middle
        mid[:, side(h)] = middle
        for s in both:
            z2[s, h] = send(xs.at[0, 0, :, side(h)], xs.at[slot(-2 * s), 0, :, side(h)], "z", 2 * s)

    def half_to_mate(s, h):
        xn[s, h] = copies.send_to(xs.at[s, 0, :, side(h)], xs.at[s, 1, :, side(h)], mate)

    def to_mate(s):
        xn[s] = copies.send_to(xs.at[s, 0], xs.at[s, 1], mate)

    def features(index):
        return pl.ds(pl.multiple_of(index * width, width), width)

    everyone = [{"y": lax.rem(y + dy, 4), "c": lax.rem(c + dc, 2)} for dy in (2, 1, 3, 0) for dc in (1, 0)]
    spread = []

    def spread_out(row_ref, place, step=0, among=None):
        for peer in among or (everyone if step else everyone[:-1]):
            other = 2 * peer["y"] + peer["c"]
            device = dict(peer, **neighbour("z", step)) if step else peer
            spread.append(copies.send_to(row_ref.at[:, features(other)], gathered.at[place, tp], device))
        if not step:
            gathered[place, tp] = row_ref[:, features(tp)]

    def halves(s):
        return (0, 1) if s > 0 else (1, 0)

    for s in both:
        z1[s] = send(xs.at[0, 0], xs.at[slot(-s), 0], "z", s)
    to_mate(0)
    first_down.wait_recv()
    along = {step: send(down_rows(0, c), down_rows(0, c), "y", step) for step in (2, 1, -1)}
    handed.append(send(down_rows(0, c), down_rows(0, c), "c", 1))
    hand_over(0)
    for h in range(heads):
        decay = decay_of(h)
        values = v_t[h * size : (h + 1) * size]

        def renew(j, carry):
            for u in range(8):
                k = 8 * j + u
                new_ref[h, k] = decay * states[h, k] + k_t[pl.ds(h * size + k, 1)] * values
            return carry

        lax.fori_loop(0, size // 8, renew, 0)
    for h in both_halves:
        for s in both:
            z2[s, h].wait_recv()
            came = slot(-2 * s)
            if h == halves(s)[0]:
                z4[s] = send(xs.at[came, 0, :, side(h)], xs.at[7, 0, :, side(h)], "z", 2 * s)
            z3[s, h] = send(xs.at[came, 0, :, side(h)], xs.at[slot(-3 * s), 0, :, side(h)], "z", s)
            half_to_mate(came, h)
    hand_over(1)
    spread_out(mid, 5)
    for s in both:
        z1[s].wait_recv()
        to_mate(slot(-s))
    for step in (2, 1, -1):
        along[step].wait_recv()
        handed.append(send(down_rows(step, c), down_rows(step, c), "c", 1))
    for s in both:
        z4[s].wait_recv()
    to_mate(7)
    for s in both:
        z3[s, 0].wait_recv()
        half_to_mate(slot(-3 * s), 0)
    for s in both:
        z3[s, 1].wait_recv()
        half_to_mate(slot(-3 * s), 1)
    gain = channel_gain_ref[...].astype(F32)

    def mix(first, stop):
        n = (stop - first) * 32
        squares = 0.0
        for i in range(D // lanes):
            cols = slice(i * lanes, (i + 1) * lanes)
            rows = xs[first:stop, :, :, cols].reshape(n, lanes).astype(F32)
            squares = squares + rows * rows
            scaled[0:n, cols] = (rows * gain[i : i + 1]).astype(BF16)
        second_rms = lax.rsqrt(jnp.sum(squares, axis=1, keepdims=True) / D + EPSILON)
        result = 0.0
        for up, down in ((up_ref, down_ref), (up_far, down_far)):
            hidden = jnp.dot(scaled[0:n], up[...], preferred_element_type=F32) * second_rms
            activated = jnp.square(jnp.maximum(hidden, 0.0)).astype(BF16)
            result = result + jnp.dot(activated, down[...], preferred_element_type=F32)
        ps[first:stop] = result.astype(BF16).reshape(stop - first, 2, 16, D)

    for copy in handed:
        copy.wait_recv()
    for key in (0, (3, 0), (4, 0), (3, 1), (4, 1), 1, 2):
        xn[key].wait_recv()
    mix(0, 5)

    xo = {}

    def back_to_mate(s):
        xo[s] = copies.send_to(ps.at[s, 1], x_in.at[s], mate)

    def with_mate(s):
        xo[s].wait_recv()
        return ps[s, 0].astype(F32) + x_in[s].astype(F32)

    for s in (3, 4, 1):
        back_to_mate(s)
    for key in (7, (5, 0), (6, 0), (5, 1), (6, 1)):
        xn[key].wait_recv()
    mix(5, 8)
    back_to_mate(7)
    turns = (2, 1, 3, 0)

    def quarter(q):
        return pl.ds(pl.multiple_of(lax.rem(y + turns[q], 4) * (D // 4), D // 4), D // 4)

    third = {}
    for q in range(4):
        for s in both:
            at, cols = slot(3 * s), quarter(q)
            third[s, q] = copies.send_to(ps.at[at, 1, :, cols], x_in.at[at, :, cols], mate)
    for s in (2, 0):
        back_to_mate(s)

    o3, o4 = {}, {}
    ps[7, 0] = with_mate(7).astype(BF16)
    farthest = {1: (0, 1), -1: (2, 3)}
    for i in range(2):
        for s in both:
            q = farthest[s][i]
            o4[s, q] = send(ps.at[7, 0, :, quarter(q)], z4_in.at[slot(s) - 1, :, quarter(q)], "z", 2 * s)
    for q in range(4):
        for s in both:
            at, cols = slot(3 * s), quarter(q)
            third[s, q].wait_recv()
            ps[at, 0, :, cols] = (ps[at, 0, :, cols].astype(F32) + x_in[at, :, cols].astype(F32)).astype(BF16)
            o3[s, q] = send(ps.at[at, 0, :, cols], z3_in.at[slot(s) - 1, :, cols], "z", s)
    for s in both:
        ps[slot(s), 0] = with_mate(slot(s)).astype(BF16)
        spread_out(ps.at[slot(s), 0], slot(s) - 1, s)
    ps[0, 0] = with_mate(0).astype(BF16)
    spread_out(ps.at[0, 0], 4)
    for s in both:
        xo[slot(2 * s)].wait_recv()
    for q in range(4):
        for s in both:
            there, cols = slot(2 * s), quarter(q)
            total = ps[there, 0, :, cols].astype(F32) + x_in[there, :, cols].astype(F32)
            if q in farthest[s]:
                o4[s, q].wait_recv()
                total = total + z4_in[slot(s) - 1, :, cols].astype(F32)
            o3[s, q].wait_recv()
            total = total + z3_in[slot(s) - 1, :, cols].astype(F32)
            ps[there, 0, :, cols] = total.astype(BF16)
            spread_out(ps.at[there, 0], slot(s) + 1, 2 * s, everyone[2 * q : 2 * q + 2])
    for copy in spread:
        copy.wait_recv()
    total = 0.0
    for place in range(6):
        total = total + gathered[place].astype(F32)
    out_ref[...] = total.astype(BF16)
    copies.finish()


def write_kernel(out_vmem, new_vmem, out_hbm, new_hbm, sem):
    copies = [pltpu.make_async_copy(out_vmem, out_hbm, sem.at[0])]
    heads, size = new_vmem.shape[0], new_vmem.shape[1]
    parts = 4
    for h in range(heads):
        for i in range(parts):
            k = slice(i * size // parts, (i + 1) * size // parts)
            copies.append(pltpu.make_async_copy(new_vmem.at[h, k], new_hbm.at[h, k], sem.at[len(copies)]))
    for copy in copies:
        copy.start()
    for copy in copies:
        copy.wait()


def write_out(out, new_states):
    vmem = pl.BlockSpec(memory_space=pltpu.VMEM)
    hbm = pl.BlockSpec(memory_space=pltpu.HBM)
    return pl.pallas_call(
        write_kernel,
        out_shape=(pltpu.HBM(out.shape, out.dtype), pltpu.HBM(new_states.shape, new_states.dtype)),
        in_specs=[vmem, vmem],
        out_specs=(hbm, hbm),
        scratch_shapes=[pltpu.SemaphoreType.DMA((9,))],
        compiler_params=pltpu.CompilerParams(vmem_limit_bytes=8 * 2**20),
        name="write_out",
    )(
        pltpu.with_memory_space_constraint(out, pltpu.VMEM),
        pltpu.with_memory_space_constraint(new_states, pltpu.VMEM),
    )


def in_hbm(array):
    return pltpu.with_memory_space_constraint(array, pltpu.HBM)


def local(
    tokens,
    states,
    mix_gain,
    w_query,
    w_key,
    w_value,
    w_gate,
    head_gain,
    w_output,
    channel_gain,
    w_up,
    w_down,
):
    rows, heads, size, _ = states.shape
    hidden = w_up.shape[1]
    angles = POS * ROTARY_BASE ** (-np.arange(size // 2) / (size // 2))
    turn = np.concatenate([np.cos(angles), np.sin(angles)]).astype(np.float32)[:, None]
    vmem = pl.BlockSpec(memory_space=pltpu.VMEM)
    hbm = pl.BlockSpec(memory_space=pltpu.HBM)
    copies = 136
    out, new_states = pl.pallas_call(
        layer_kernel,
        out_shape=(
            pltpu.VMEM((8, 16, tokens.shape[1]), BF16),
            pltpu.VMEM((heads, size, size, rows), F32),
        ),
        in_specs=[hbm] * 13,
        out_specs=(vmem, vmem),
        scratch_shapes=[
            pltpu.VMEM((D // 128, 128), BF16),
            pltpu.VMEM((1, heads * size), BF16),
            pltpu.VMEM((D // 128, 128), BF16),
            pltpu.VMEM((size, 1), F32),
            pltpu.VMEM((8, rows, tokens.shape[1]), BF16),
            pltpu.VMEM((D, 4 * heads * size), BF16),
            pltpu.VMEM((heads * size, D), BF16),
            pltpu.VMEM((heads, size, size, rows), F32),
            pltpu.VMEM((rows, 4 * heads * size), F32),
            pltpu.VMEM((D // 128, 128), F32),
            pltpu.VMEM((heads * size, rows), F32),
            pltpu.VMEM((heads * size, rows), F32),
            pltpu.VMEM((heads * size, rows), F32),
            pltpu.VMEM((heads * size, rows), F32),
            pltpu.VMEM((4, 2, 16, heads * size), BF16),
            pltpu.VMEM((4, 16, heads * size), BF16),
            pltpu.VMEM((heads * size, D), BF16),
            pltpu.VMEM((4, 16, D), BF16),
            pltpu.VMEM((D, hidden), BF16),
            pltpu.VMEM((hidden, D), BF16),
            pltpu.VMEM((D, hidden), BF16),
            pltpu.VMEM((hidden, D), BF16),
            pltpu.VMEM((8, 2, 16, D), BF16),
            pltpu.VMEM((8, 2, 16, D), BF16),
            pltpu.VMEM((160, D), BF16),
            pltpu.VMEM((3, 16, D), BF16),
            pltpu.VMEM((16, D), BF16),
            pltpu.VMEM((8, 16, D), BF16),
            pltpu.VMEM((2, 16, D), BF16),
            pltpu.VMEM((2, 16, D), BF16),
            pltpu.VMEM((6, 8, 16, tokens.shape[1]), BF16),
            pltpu.SemaphoreType.DMA((12,)),
            pltpu.SemaphoreType.DMA((heads * size // 16,)),
            pltpu.SemaphoreType.DMA((copies,)),
            pltpu.SemaphoreType.DMA((copies,)),
        ],
        compiler_params=pltpu.CompilerParams(
            collective_id=0, has_side_effects=True, vmem_limit_bytes=40 * 2**20
        ),
        name="layer",
    )(
        in_hbm(tokens),
        in_hbm(states.transpose(1, 2, 3, 0)),
        in_hbm(mix_gain.reshape(D // 128, 128)),
        in_hbm(w_query),
        in_hbm(w_key),
        in_hbm(w_value),
        in_hbm(w_gate),
        in_hbm(head_gain.reshape(1, heads * size)),
        in_hbm(w_output),
        in_hbm(channel_gain.reshape(D // 128, 128)),
        in_hbm(w_up),
        in_hbm(w_down),
        in_hbm(jnp.asarray(turn)),
    )
    out, new_states = write_out(out, new_states)
    return (out.reshape(tokens.shape), new_states.transpose(3, 0, 1, 2))


def solution(mesh):
    torus = Mesh(mesh.devices.reshape(8, 4, 4, 2), ("z", "x", "y", "c"))
    in_specs = (
        P(KV, TP),
        P(KV, TP, None, None),
        P(),
        P(None, TP),
        P(None, TP),
        P(None, TP),
        P(None, TP),
        P(TP),
        P(TP, None),
        P(),
        P(None, KV),
        P(KV, None),
    )
    out_specs = (P(KV, TP), P(KV, TP, None, None))
    return jax.shard_map(local, mesh=torus, in_specs=in_specs, out_specs=out_specs, check_vma=False)
```

```python
import jax
import jax.numpy as jnp
import numpy as np
from jax import lax
from jax.experimental import pallas as pl
from jax.experimental.pallas import tpu as pltpu
from jax.sharding import Mesh
from jax.sharding import PartitionSpec as P

HEADS = 16
POS = 16384
KV = ("z", "x")
TP = ("y", "c")

EPSILON = 1e-06
ROTARY_BASE = 10000.0

D = 2048
SIZES = {"z": 8, "x": 4, "y": 4, "c": 2}
F32 = jnp.float32
BF16 = jnp.bfloat16


def slot(offset):
    return 2 * abs(offset) - (1 if offset > 0 else 0)


class Copies:
    def __init__(self, send_sem, recv_sem):
        self.send_sem, self.recv_sem, self.made = send_sem, recv_sem, []

    def send_to(self, src, dst, device):
        index = len(self.made)
        copy = pltpu.make_async_remote_copy(
            src_ref=src,
            dst_ref=dst,
            send_sem=self.send_sem.at[index],
            recv_sem=self.recv_sem.at[index],
            device_id=device,
            device_id_type=pl.DeviceIdType.MESH,
        )
        copy.start()
        self.made.append(copy)
        return copy

    def send(self, src, dst, axis, step):
        return self.send_to(src, dst, neighbour(axis, step))

    def finish(self):
        for copy in self.made:
            copy.wait_send()


def greet(peers):
    barrier = pltpu.get_barrier_semaphore()
    for peer in peers:
        pl.semaphore_signal(barrier, inc=1, device_id=peer, device_id_type=pl.DeviceIdType.MESH)
    return barrier


def neighbour(axis, step):
    n = SIZES[axis]
    return {axis: lax.rem(lax.axis_index(axis) + (step + n), n)}


def half(start, stop, step):
    middle = (start + stop) // 2
    return slice(start, middle) if step > 0 else slice(middle, stop)


def layer_kernel(
    tok_hbm,
    states_hbm,
    mix_gain_hbm,
    wq_hbm,
    wk_hbm,
    wv_hbm,
    wg_hbm,
    head_gain_hbm,
    wo_hbm,
    channel_gain_hbm,
    up_hbm,
    down_hbm,
    turn_hbm,
    out_ref,
    new_ref,
    mix_gain_ref,
    head_gain_ref,
    channel_gain_ref,
    turn_ref,
    blocks,
    w_ref,
    wo_ref,
    states,
    projected,
    gain_rows,
    q_t,
    k_t,
    v_t,
    gated_t,
    gated_rows,
    gated_in,
    wo_pair,
    part,
    up_ref,
    down_ref,
    up_far,
    down_far,
    xs,
    ps,
    scaled,
    y_in,
    mid,
    x_in,
    z3_in,
    z4_in,
    gathered,
    load_sem,
    state_sem,
    send_sem,
    recv_sem,
):
    x, y, c = lax.axis_index("x"), lax.axis_index("y"), lax.axis_index("c")
    tp = 2 * y + c
    both = (1, -1)
    mate = {"x": lax.rem(x + 1 + 2 * lax.rem(x + c, 2), 4)}
    peers = [{"y": lax.rem(y + dy, 4), "c": lax.rem(c + dc, 2)} for dy in range(4) for dc in range(2) if dy or dc]
    ring = [neighbour("z", step) for step in (1, -1, 2, -2)] + [mate, neighbour("x", 2)]
    barrier = greet(peers + ring)

    heads, size = states.shape[0], states.shape[1]
    chunk = 16
    spans = [(h, slice(k, k + chunk)) for h in range(heads) for k in range(0, size, chunk)]
    load_tok = pltpu.make_async_copy(tok_hbm, blocks.at[tp], load_sem.at[0])
    load_up = pltpu.make_async_copy(up_hbm, up_ref, load_sem.at[1])
    load_down = pltpu.make_async_copy(down_hbm, down_ref, load_sem.at[2])
    load_w = []
    for i, w in enumerate((wq_hbm, wk_hbm, wv_hbm, wg_hbm)):
        load_w.append(pltpu.make_async_copy(w, w_ref.at[:, 128 * i : 128 * (i + 1)], load_sem.at[3 + i]))
    load_out = pltpu.make_async_copy(wo_hbm, wo_ref, load_sem.at[7])
    load_states = []
    for i, (h, k) in enumerate(spans):
        load_states.append(pltpu.make_async_copy(states_hbm.at[h, k], states.at[h, k], state_sem.at[i]))
    small = ((mix_gain_hbm, mix_gain_ref), (head_gain_hbm, head_gain_ref), (channel_gain_hbm, channel_gain_ref), (turn_hbm, turn_ref))
    load_small = [pltpu.make_async_copy(src, dst, load_sem.at[8 + i]) for i, (src, dst) in enumerate(small)]
    for copy in [load_tok, load_up, load_down] + load_small + load_w + load_states + [load_out]:
        copy.start()
    load_tok.wait()
    pl.semaphore_wait(barrier, len(peers) + len(ring))

    copies = Copies(send_sem, recv_sem)
    send = copies.send

    own = blocks.at[tp]
    near = {step: send(own, own, "y", step) for step in (1, -1, 2)}
    across = [send(own, own, "c", 1)]

    load_up.wait()
    load_down.wait()
    eighth = down_ref.shape[0] // 8

    def down_rows(step, core):
        block = 2 * lax.rem(y + (4 - step), 4) + core
        return down_far.at[pl.ds(pl.multiple_of(block * eighth, eighth), eighth)]

    first_down = send(down_ref.at[pl.ds(pl.multiple_of(tp * eighth, eighth), eighth)], down_rows(0, c), "x", 2)
    weights = []
    deep = up_ref.shape[0] // 4
    for i in range(2):
        rows = pl.ds(pl.multiple_of((2 * c + i) * deep, deep), deep)
        weights.append((up_far.at[rows], send(up_ref.at[rows], up_far.at[rows], "x", 2)))
    load_out.wait()
    pair_out = send(wo_ref, wo_pair, "c", 1)
    handed = []

    def hand_over(i):
        there, copy = weights[i]
        copy.wait_recv()
        handed.append(send(there, there, "c", 1))

    width = blocks.shape[2]
    lanes = 128
    for copy in load_small + load_w:
        copy.wait()
    gain_rows[...] = mix_gain_ref[...].astype(F32)

    def project(index, squares):
        block = blocks[index].astype(F32)
        gains = [gain_rows[pl.ds(index * (width // lanes) + i, 1)] for i in range(width // lanes)]
        scaled_block = (block * jnp.concatenate(gains, axis=1)).astype(BF16)
        rows = pl.ds(pl.multiple_of(index * width, width), width)
        product = jnp.dot(scaled_block, w_ref[rows], preferred_element_type=F32)
        if squares is None:
            projected[...] = product
            return jnp.sum(block * block, axis=1, keepdims=True)
        projected[...] += product
        return squares + jnp.sum(block * block, axis=1, keepdims=True)

    def block_of(step, core):
        return 2 * lax.rem(y + (4 - step), 4) + core

    total = project(tp, None)
    for step in (1, -1, 2):
        near[step].wait_recv()
        arrived = blocks.at[block_of(step, c)]
        across.append(send(arrived, arrived, "c", 1))
    for step in (1, -1, 2):
        total = project(block_of(step, c), total)
    for i, step in enumerate((0, 1, -1, 2)):
        across[i].wait_recv()
        total = project(block_of(step, 1 - c), total)
    inverse_rms = lax.rsqrt(total / D + EPSILON)

    turned = [(projected[:, 128 * i : 128 * (i + 1)] * inverse_rms).T for i in range(4)]
    cosine, sines = turn_ref[0 : size // 2], turn_ref[size // 2 : size]
    for source, target, scale in ((turned[0], q_t, size ** (-0.5)), (turned[1], k_t, 1.0)):
        for h in range(heads):
            first = source[h * size : h * size + size // 2]
            second = source[h * size + size // 2 : (h + 1) * size]
            target[h * size : h * size + size // 2] = (first * cosine - second * sines) * scale
            target[h * size + size // 2 : (h + 1) * size] = (first * sines + second * cosine) * scale
    v_t[...] = turned[2]

    def decay_of(h):
        head = jnp.full((1, lanes), heads * tp + h).astype(F32)
        return 1.0 - jnp.exp2(-1.0 - 11.0 * head / (HEADS - 1))

    for h in range(heads):
        rows = slice(h * size, (h + 1) * size)
        values = turned[2][rows]
        sums = jnp.zeros_like(values)
        for i, (span_head, ks) in enumerate(spans):
            if span_head != h:
                continue
            load_states[i].wait()

            def step(j, sums):
                for u in range(8):
                    k = ks.start + 8 * j + u
                    sums = sums + q_t[pl.ds(h * size + k, 1)] * states[h, k]
                return sums

            sums = lax.fori_loop(0, chunk // 8, step, sums)
        overlap = jnp.sum(q_t[rows] * k_t[rows], axis=0, keepdims=True)
        output = decay_of(h) * sums + overlap * values
        center = output - jnp.mean(output, axis=0, keepdims=True)
        spread = jnp.mean(center * center, axis=0, keepdims=True)
        gate = turned[3][rows]
        gated_t[rows] = center * lax.rsqrt(spread + EPSILON) * (gate * jax.nn.sigmoid(gate))
    gated = (gated_t[...].T * head_gain_ref[...].astype(F32)).astype(BF16)
    gated_rows[...] = gated.reshape(4, 2, 16, heads * size)

    traded = send(gated_rows.at[:, 1 - c], gated_in, "c", 1)

    def side(h):
        return slice(h * D // 2, (h + 1) * D // 2)

    offsets = (2, 1, -1)
    near = {}
    own_gated = gated_rows[:, c].reshape(64, heads * size)
    firsts = [jnp.dot(own_gated, wo_ref[:, side(h)], preferred_element_type=F32) for h in range(2)]
    pair_out.wait_recv()
    traded.wait_recv()
    other_gated = gated_in[...].reshape(64, heads * size)
    for h in range(2):
        product = firsts[h] + jnp.dot(other_gated, wo_pair[:, side(h)], preferred_element_type=F32)
        part[:, :, side(h)] = product.astype(BF16).reshape(4, 16, D // 2)
        for i, o in enumerate(offsets):
            there = part.at[lax.rem(y + (o + 4), 4), :, side(h)]
            near[i, h] = send(there, y_in.at[i, :, side(h)], "y", o)
    mine = pl.ds(pl.multiple_of(16 * tp, 16), 16)
    own_rows = jnp.concatenate([blocks[i, mine] for i in range(8)], axis=1).astype(F32)
    z1, z2, z3, z4, xn = {}, {}, {}, {}, {}
    both_halves = (0, 1)
    for h in both_halves:
        attended = part[y, :, side(h)].astype(F32)
        for i in (1, 2, 0):
            near[i, h].wait_recv()
            attended = attended + y_in[i, :, side(h)].astype(F32)
        middle = (own_rows[:, side(h)] + attended).astype(BF16)
        xs[0, 0, :, side(h)] = middle
        mid[:, side(h)] = middle
        for s in both:
            z2[s, h] = send(xs.at[0, 0, :, side(h)], xs.at[slot(-2 * s), 0, :, side(h)], "z", 2 * s)
        xn[0, h] = copies.send_to(xs.at[0, 0, :, side(h)], xs.at[0, 1, :, side(h)], mate)

    def half_to_mate(s, h):
        xn[s, h] = copies.send_to(xs.at[s, 0, :, side(h)], xs.at[s, 1, :, side(h)], mate)

    def to_mate(s):
        xn[s] = copies.send_to(xs.at[s, 0], xs.at[s, 1], mate)

    def features(index):
        return pl.ds(pl.multiple_of(index * width, width), width)

    everyone = [{"y": lax.rem(y + dy, 4), "c": lax.rem(c + dc, 2)} for dy in (2, 1, 3, 0) for dc in (1, 0)]
    spread = []

    def spread_out(row_ref, place, step=0, among=None):
        for peer in among or (everyone if step else everyone[:-1]):
            other = 2 * peer["y"] + peer["c"]
            device = dict(peer, **neighbour("z", step)) if step else peer
            spread.append(copies.send_to(row_ref.at[:, features(other)], gathered.at[place, tp], device))
        if not step:
            gathered[place, tp] = row_ref[:, features(tp)]

    def halves(s):
        return (0, 1) if s > 0 else (1, 0)

    for s in both:
        z1[s] = send(xs.at[0, 0], xs.at[slot(-s), 0], "z", s)
    first_down.wait_recv()
    along = {step: send(down_rows(0, c), down_rows(0, c), "y", step) for step in (2, 1, -1)}
    handed.append(send(down_rows(0, c), down_rows(0, c), "c", 1))
    hand_over(0)
    for h in range(heads):
        decay = decay_of(h)
        values = v_t[h * size : (h + 1) * size]

        def renew(j, carry):
            for u in range(8):
                k = 8 * j + u
                new_ref[h, k] = decay * states[h, k] + k_t[pl.ds(h * size + k, 1)] * values
            return carry

        lax.fori_loop(0, size // 8, renew, 0)
    for h in both_halves:
        for s in both:
            z2[s, h].wait_recv()
            came = slot(-2 * s)
            if h == halves(s)[0]:
                z4[s] = send(xs.at[came, 0, :, side(h)], xs.at[7, 0, :, side(h)], "z", 2 * s)
            z3[s, h] = send(xs.at[came, 0, :, side(h)], xs.at[slot(-3 * s), 0, :, side(h)], "z", s)
            half_to_mate(came, h)
    hand_over(1)
    spread_out(mid, 5)
    for s in both:
        z1[s].wait_recv()
        to_mate(slot(-s))
    for step in (2, 1, -1):
        along[step].wait_recv()
        handed.append(send(down_rows(step, c), down_rows(step, c), "c", 1))
    for s in both:
        z4[s].wait_recv()
    to_mate(7)
    for s in both:
        z3[s, 0].wait_recv()
        half_to_mate(slot(-3 * s), 0)
    for s in both:
        z3[s, 1].wait_recv()
        half_to_mate(slot(-3 * s), 1)
    gain = channel_gain_ref[...].astype(F32)

    def mix(first, stop):
        n = (stop - first) * 32
        squares = 0.0
        for i in range(D // lanes):
            cols = slice(i * lanes, (i + 1) * lanes)
            rows = xs[first:stop, :, :, cols].reshape(n, lanes).astype(F32)
            squares = squares + rows * rows
            scaled[0:n, cols] = (rows * gain[i : i + 1]).astype(BF16)
        second_rms = lax.rsqrt(jnp.sum(squares, axis=1, keepdims=True) / D + EPSILON)
        result = 0.0
        for up, down in ((up_ref, down_ref), (up_far, down_far)):
            hidden = jnp.dot(scaled[0:n], up[...], preferred_element_type=F32) * second_rms
            activated = jnp.square(jnp.maximum(hidden, 0.0)).astype(BF16)
            result = result + jnp.dot(activated, down[...], preferred_element_type=F32)
        ps[first:stop] = result.astype(BF16).reshape(stop - first, 2, 16, D)

    for copy in handed:
        copy.wait_recv()
    for key in ((0, 0), (0, 1), (3, 0), (4, 0), (3, 1), (4, 1), 1, 2):
        xn[key].wait_recv()
    mix(0, 5)

    xo = {}

    def back_to_mate(s):
        xo[s] = copies.send_to(ps.at[s, 1], x_in.at[s], mate)

    def with_mate(s):
        xo[s].wait_recv()
        return ps[s, 0].astype(F32) + x_in[s].astype(F32)

    for s in (3, 4, 1):
        back_to_mate(s)
    for key in (7, (5, 0), (6, 0), (5, 1), (6, 1)):
        xn[key].wait_recv()
    mix(5, 8)
    back_to_mate(7)
    turns = (2, 1, 3, 0)

    def quarter(q):
        return pl.ds(pl.multiple_of(lax.rem(y + turns[q], 4) * (D // 4), D // 4), D // 4)

    third = {}
    for q in range(4):
        for s in both:
            at, cols = slot(3 * s), quarter(q)
            third[s, q] = copies.send_to(ps.at[at, 1, :, cols], x_in.at[at, :, cols], mate)
    for s in (2, 0):
        back_to_mate(s)

    o3, o4 = {}, {}
    ps[7, 0] = with_mate(7).astype(BF16)
    farthest = {1: (0, 1), -1: (2, 3)}
    for i in range(2):
        for s in both:
            q = farthest[s][i]
            o4[s, q] = send(ps.at[7, 0, :, quarter(q)], z4_in.at[slot(s) - 1, :, quarter(q)], "z", 2 * s)
    for q in range(4):
        for s in both:
            at, cols = slot(3 * s), quarter(q)
            third[s, q].wait_recv()
            ps[at, 0, :, cols] = (ps[at, 0, :, cols].astype(F32) + x_in[at, :, cols].astype(F32)).astype(BF16)
            o3[s, q] = send(ps.at[at, 0, :, cols], z3_in.at[slot(s) - 1, :, cols], "z", s)
    for s in both:
        ps[slot(s), 0] = with_mate(slot(s)).astype(BF16)
        spread_out(ps.at[slot(s), 0], slot(s) - 1, s)
    ps[0, 0] = with_mate(0).astype(BF16)
    spread_out(ps.at[0, 0], 4)
    for s in both:
        xo[slot(2 * s)].wait_recv()
    for q in range(4):
        for s in both:
            there, cols = slot(2 * s), quarter(q)
            total = ps[there, 0, :, cols].astype(F32) + x_in[there, :, cols].astype(F32)
            if q in farthest[s]:
                o4[s, q].wait_recv()
                total = total + z4_in[slot(s) - 1, :, cols].astype(F32)
            o3[s, q].wait_recv()
            total = total + z3_in[slot(s) - 1, :, cols].astype(F32)
            ps[there, 0, :, cols] = total.astype(BF16)
            spread_out(ps.at[there, 0], slot(s) + 1, 2 * s, everyone[2 * q : 2 * q + 2])
    for copy in spread:
        copy.wait_recv()
    total = 0.0
    for place in range(6):
        total = total + gathered[place].astype(F32)
    out_ref[...] = total.astype(BF16)
    copies.finish()


def write_kernel(out_vmem, new_vmem, out_hbm, new_hbm, sem):
    copies = [pltpu.make_async_copy(out_vmem, out_hbm, sem.at[0])]
    heads, size = new_vmem.shape[0], new_vmem.shape[1]
    parts = 4
    for h in range(heads):
        for i in range(parts):
            k = slice(i * size // parts, (i + 1) * size // parts)
            copies.append(pltpu.make_async_copy(new_vmem.at[h, k], new_hbm.at[h, k], sem.at[len(copies)]))
    for copy in copies:
        copy.start()
    for copy in copies:
        copy.wait()


def write_out(out, new_states):
    vmem = pl.BlockSpec(memory_space=pltpu.VMEM)
    hbm = pl.BlockSpec(memory_space=pltpu.HBM)
    return pl.pallas_call(
        write_kernel,
        out_shape=(pltpu.HBM(out.shape, out.dtype), pltpu.HBM(new_states.shape, new_states.dtype)),
        in_specs=[vmem, vmem],
        out_specs=(hbm, hbm),
        scratch_shapes=[pltpu.SemaphoreType.DMA((9,))],
        compiler_params=pltpu.CompilerParams(vmem_limit_bytes=8 * 2**20),
        name="write_out",
    )(
        pltpu.with_memory_space_constraint(out, pltpu.VMEM),
        pltpu.with_memory_space_constraint(new_states, pltpu.VMEM),
    )


def in_hbm(array):
    return pltpu.with_memory_space_constraint(array, pltpu.HBM)


def local(
    tokens,
    states,
    mix_gain,
    w_query,
    w_key,
    w_value,
    w_gate,
    head_gain,
    w_output,
    channel_gain,
    w_up,
    w_down,
):
    rows, heads, size, _ = states.shape
    hidden = w_up.shape[1]
    angles = POS * ROTARY_BASE ** (-np.arange(size // 2) / (size // 2))
    turn = np.concatenate([np.cos(angles), np.sin(angles)]).astype(np.float32)[:, None]
    vmem = pl.BlockSpec(memory_space=pltpu.VMEM)
    hbm = pl.BlockSpec(memory_space=pltpu.HBM)
    copies = 136
    out, new_states = pl.pallas_call(
        layer_kernel,
        out_shape=(
            pltpu.VMEM((8, 16, tokens.shape[1]), BF16),
            pltpu.VMEM((heads, size, size, rows), F32),
        ),
        in_specs=[hbm] * 13,
        out_specs=(vmem, vmem),
        scratch_shapes=[
            pltpu.VMEM((D // 128, 128), BF16),
            pltpu.VMEM((1, heads * size), BF16),
            pltpu.VMEM((D // 128, 128), BF16),
            pltpu.VMEM((size, 1), F32),
            pltpu.VMEM((8, rows, tokens.shape[1]), BF16),
            pltpu.VMEM((D, 4 * heads * size), BF16),
            pltpu.VMEM((heads * size, D), BF16),
            pltpu.VMEM((heads, size, size, rows), F32),
            pltpu.VMEM((rows, 4 * heads * size), F32),
            pltpu.VMEM((D // 128, 128), F32),
            pltpu.VMEM((heads * size, rows), F32),
            pltpu.VMEM((heads * size, rows), F32),
            pltpu.VMEM((heads * size, rows), F32),
            pltpu.VMEM((heads * size, rows), F32),
            pltpu.VMEM((4, 2, 16, heads * size), BF16),
            pltpu.VMEM((4, 16, heads * size), BF16),
            pltpu.VMEM((heads * size, D), BF16),
            pltpu.VMEM((4, 16, D), BF16),
            pltpu.VMEM((D, hidden), BF16),
            pltpu.VMEM((hidden, D), BF16),
            pltpu.VMEM((D, hidden), BF16),
            pltpu.VMEM((hidden, D), BF16),
            pltpu.VMEM((8, 2, 16, D), BF16),
            pltpu.VMEM((8, 2, 16, D), BF16),
            pltpu.VMEM((160, D), BF16),
            pltpu.VMEM((3, 16, D), BF16),
            pltpu.VMEM((16, D), BF16),
            pltpu.VMEM((8, 16, D), BF16),
            pltpu.VMEM((2, 16, D), BF16),
            pltpu.VMEM((2, 16, D), BF16),
            pltpu.VMEM((6, 8, 16, tokens.shape[1]), BF16),
            pltpu.SemaphoreType.DMA((12,)),
            pltpu.SemaphoreType.DMA((heads * size // 16,)),
            pltpu.SemaphoreType.DMA((copies,)),
            pltpu.SemaphoreType.DMA((copies,)),
        ],
        compiler_params=pltpu.CompilerParams(
            collective_id=0, has_side_effects=True, vmem_limit_bytes=40 * 2**20
        ),
        name="layer",
    )(
        in_hbm(tokens),
        in_hbm(states.transpose(1, 2, 3, 0)),
        in_hbm(mix_gain.reshape(D // 128, 128)),
        in_hbm(w_query),
        in_hbm(w_key),
        in_hbm(w_value),
        in_hbm(w_gate),
        in_hbm(head_gain.reshape(1, heads * size)),
        in_hbm(w_output),
        in_hbm(channel_gain.reshape(D // 128, 128)),
        in_hbm(w_up),
        in_hbm(w_down),
        in_hbm(jnp.asarray(turn)),
    )
    out, new_states = write_out(out, new_states)
    return (out.reshape(tokens.shape), new_states.transpose(3, 0, 1, 2))


def solution(mesh):
    torus = Mesh(mesh.devices.reshape(8, 4, 4, 2), ("z", "x", "y", "c"))
    in_specs = (
        P(KV, TP),
        P(KV, TP, None, None),
        P(),
        P(None, TP),
        P(None, TP),
        P(None, TP),
        P(None, TP),
        P(TP),
        P(TP, None),
        P(),
        P(None, KV),
        P(KV, None),
    )
    out_specs = (P(KV, TP), P(KV, TP, None, None))
    return jax.shard_map(local, mesh=torus, in_specs=in_specs, out_specs=out_specs, check_vma=False)
```
